512 devices in a mesh: sp: 64 (over z, y), tp: 8 (over x, core).
Axes of the slice: x: 4, y: 8, z: 8, core: 2. Of those that a mesh axis runs over, the one named last changes fastest.
Arguments:
- latent_tokens: bfloat16 [8192, 2048], P(('sp', 'tp')), may hold values from -6 to 6
- context_tokens: bfloat16 [512, 2048], P('sp'), may hold values from -6 to 6
- cond: float32 [2048], replicated, may hold values from -6 to 6
- ctx_cond: float32 [2048], replicated, may hold values from -6 to 6
- mod_shift: bfloat16 [2048, 2048], P('sp', 'tp'), may hold values from -0.125 to 0.125
- mod_scale: bfloat16 [2048, 2048], P('sp', 'tp'), may hold values from -0.125 to 0.125
- mod_gate: bfloat16 [2048, 2048], P('sp', 'tp'), may hold values from -0.125 to 0.125
- norm_gain: float32 [2048], replicated, may hold values from 0.1 to 1.9
- w_query: bfloat16 [2048, 1536], P(None, 'tp'), may hold values from -0.125 to 0.125
- query_gain: float32 [96], replicated, may hold values from 0.8 to 2
- w_down_kv: bfloat16 [2048, 256], replicated, may hold values from -0.125 to 0.125
- w_rope_key: bfloat16 [2048, 32], replicated, may hold values from -0.125 to 0.125
- kv_gain: float32 [256], replicated, may hold values from 0.1 to 1.9
- w_up_kv: bfloat16 [2, 256, 1024], P(None, None, 'tp'), may hold values from -0.375 to 0.375
- key_gain: float32 [96], replicated, may hold values from 0.8 to 2
- ctx_lift: float32 [16], P('tp'), may hold values from 1.5 to 220
- w_output: bfloat16 [1024, 2048], P('tp'), may hold values from -0.1875 to 0.1875
Outputs:
- updated: bfloat16 [8192, 2048], P(('sp', 'tp'))
The draws below stay inside these ranges and needn't reach their ends.
All inputs are finite; a program needn't handle non-finite values.
Results may differ from the reference program's by a relative error of at most 0.007.
Values may be sent and summed in bfloat16 or wider, within the bound.
A program may use at most 64 MiB of HBM per device.

```python
import math
import jax
import jax.numpy as jnp
from jax import lax

D = 2048
HEADS = 16
HD = 64
ROPE = 32
KVL = 256
QK = 96
SEQ = 8192
CTX = 512
GRID_W = 64


def draw_ctx_lift(key, part):
    drawn = jax.random.uniform(jax.random.fold_in(key, 11), (HEADS,), jnp.float32, 1.5, 3.5)
    return drawn


def block_levels(rng, extent, split, smallest, high):
    gain = 1.0
    for dim, blocks in split:
        draws = jax.random.uniform(jax.random.fold_in(jax.random.fold_in(rng, 6), dim), (blocks,), jnp.float32, smallest / len(split), high / len(split))
        gain = gain * jnp.repeat(jnp.exp(draws), extent[dim] // blocks).reshape((-1,) + (1,) * (len(extent) - 1 - dim))
    return gain


def centred(stream_key, extent, deviation, reach, shards=(), held_as=jnp.bfloat16):
    array = jax.random.normal(stream_key, extent, jnp.float32) * deviation
    if len(shards) > 0:
        array = block_levels(stream_key, extent, shards, -0.22, 0.18) * array
    return jnp.clip(array, min=-reach, max=reach).astype(held_as)


def setup_inputs(seed: int = 0) -> dict:
    seeds = jax.random.split(jax.random.key(seed), 18)
    latent_tokens = centred(seeds[0], (SEQ, D), 1.0, 6.0, ((0, 512),))
    context_tokens = centred(seeds[1], (CTX, D), 1.0, 6.0, ((0, 64),))
    cond = centred(seeds[2], (D,), 1.0, 6.0, (), jnp.float32)
    ctx_cond = centred(seeds[3], (D,), 1.0, 6.0, (), jnp.float32)
    mod_shift = centred(seeds[4], (D, D), D ** -0.5, 0.125, ((0, 64), (1, 8)))
    mod_scale = centred(seeds[5], (D, D), D ** -0.5, 0.125, ((0, 64), (1, 8)))
    mod_gate = centred(seeds[6], (D, D), D ** -0.5, 0.125, ((0, 64), (1, 8)))
    norm_gain = jnp.clip(1.0 + 0.18 * jax.random.normal(seeds[7], (D,), jnp.float32), 0.1, 1.9)
    w_query = centred(seeds[8], (D, HEADS * QK), D ** -0.5, 0.125, ((1, 8),))
    query_gain = jnp.clip(jnp.exp(jax.random.uniform(seeds[9], (QK,), jnp.float32, math.log(0.8), math.log(2.0))), 0.8, 2.0)
    w_down_kv = centred(seeds[10], (D, KVL), D ** -0.5, 0.125)
    w_rope_key = centred(seeds[11], (D, ROPE), D ** -0.5, 0.125)
    kv_gain = jnp.clip(1.0 + 0.18 * jax.random.normal(seeds[12], (KVL,), jnp.float32), 0.1, 1.9)
    w_up_kv = centred(seeds[13], (2, KVL, HEADS * HD), KVL ** -0.5, 0.375, ((2, 8),))
    key_gain = jnp.clip(jnp.exp(jax.random.uniform(seeds[14], (QK,), jnp.float32, math.log(0.8), math.log(2.0))), 0.8, 2.0)
    ctx_lift = draw_ctx_lift(jax.random.fold_in(seeds[17], 71), 0)
    w_output = centred(seeds[16], (HEADS * HD, D), (HEADS * HD) ** -0.5, 0.1875, ((0, 8),))
    return dict(latent_tokens=latent_tokens, context_tokens=context_tokens, cond=cond, ctx_cond=ctx_cond, mod_shift=mod_shift, mod_scale=mod_scale, mod_gate=mod_gate, norm_gain=norm_gain, w_query=w_query, query_gain=query_gain, w_down_kv=w_down_kv, w_rope_key=w_rope_key, kv_gain=kv_gain, w_up_kv=w_up_kv, key_gain=key_gain, ctx_lift=ctx_lift, w_output=w_output)


EPS = 1e-06
THETA = 10000.0

def rms_normed(values, gain_vector):
    values = values.astype(jnp.float32)
    inv_root = lax.rsqrt(lax.optimization_barrier(jnp.mean(values * values, axis=-1, keepdims=True)) + EPS)
    return values * inv_root * gain_vector

def grid_angles(position, width):
    freq_count = width // 4
    inverse = THETA ** (-jnp.arange(freq_count, dtype=jnp.float32) / freq_count)
    row_index = (position // GRID_W).astype(jnp.float32)
    col_index = (position % GRID_W).astype(jnp.float32)
    return jnp.concatenate([row_index[:, None] * inverse, col_index[:, None] * inverse], axis=-1)

def rotate_tail(head_rows, angle, plain):
    tail = head_rows[..., plain:]
    half_width = tail.shape[-1] // 2
    cosine = jnp.cos(angle)[:, None, :]
    sine_val = jnp.sin(angle)[:, None, :]
    front_half = tail[..., :half_width]
    back_half = tail[..., half_width:]
    return jnp.concatenate([head_rows[..., :plain], front_half * cosine - back_half * sine_val, back_half * cosine + front_half * sine_val], axis=-1)

def modulation(signal, weight):
    return jnp.dot(signal, weight.astype(jnp.float32), precision=lax.Precision.HIGHEST)

def compress(hidden, w_down_kv, w_rope_key, kv_gain):
    latent = rms_normed(jnp.dot(hidden, w_down_kv, preferred_element_type=jnp.float32), kv_gain)
    rope_key = jnp.dot(hidden, w_rope_key, preferred_element_type=jnp.float32)
    return (latent.astype(jnp.bfloat16), rope_key.astype(jnp.bfloat16))

def expand(latent, rope_key, w_up_kv, key_gain, angle):
    row_count = latent.shape[0]
    head_count = w_up_kv.shape[2] // HD
    key_plain = jnp.dot(latent, w_up_kv[0], preferred_element_type=jnp.float32).reshape(row_count, head_count, HD)
    shared = jnp.broadcast_to(rope_key.astype(jnp.float32)[:, None, :], (row_count, head_count, ROPE))
    keys = rms_normed(jnp.concatenate([key_plain, shared], axis=-1), key_gain)
    if angle is not None:
        keys = rotate_tail(keys, angle, HD)
    values = jnp.dot(latent, w_up_kv[1], preferred_element_type=jnp.float32).astype(jnp.bfloat16)
    return (keys.astype(jnp.bfloat16), values.reshape(row_count, head_count, HD))

def reference(latent_tokens, context_tokens, cond, ctx_cond, mod_shift, mod_scale, mod_gate, norm_gain, w_query, query_gain, w_down_kv, w_rope_key, kv_gain, w_up_kv, key_gain, ctx_lift, w_output):
    lat_signal = jax.nn.silu(cond)
    ctx_signal = jax.nn.silu(ctx_cond)
    shift_lat = modulation(lat_signal, mod_shift)
    scale_lat = modulation(lat_signal, mod_scale)
    gate_lat = modulation(lat_signal, mod_gate)
    shift_ctx = modulation(ctx_signal, mod_shift)
    scale_ctx = modulation(ctx_signal, mod_scale)
    hidden_lat = (rms_normed(latent_tokens, norm_gain) * (1.0 + scale_lat) + shift_lat).astype(jnp.bfloat16)
    hidden_ctx = (rms_normed(context_tokens, norm_gain) * (1.0 + scale_ctx) + shift_ctx).astype(jnp.bfloat16)
    position = jnp.arange(SEQ, dtype=jnp.int32)
    angle = grid_angles(position, ROPE)
    queries = jnp.dot(hidden_lat, w_query, preferred_element_type=jnp.float32).reshape(SEQ, HEADS, QK)
    queries = rotate_tail(rms_normed(queries, query_gain), angle, HD).astype(jnp.bfloat16)
    lat_latent, lat_rope = compress(hidden_lat, w_down_kv, w_rope_key, kv_gain)
    ctx_latent, ctx_rope = compress(hidden_ctx, w_down_kv, w_rope_key, kv_gain)
    lat_keys, lat_values = expand(lat_latent, lat_rope, w_up_kv, key_gain, angle)
    ctx_keys, ctx_values = expand(ctx_latent, ctx_rope, w_up_kv, key_gain, None)
    all_keys = jnp.concatenate([ctx_keys, lat_keys], axis=0).astype(jnp.float32)
    all_values = jnp.concatenate([ctx_values, lat_values], axis=0).astype(jnp.float32)
    lift = jnp.concatenate([jnp.broadcast_to(ctx_lift[:, None], (HEADS, CTX)), jnp.zeros((HEADS, SEQ), jnp.float32)], axis=1)
    block = math.gcd(SEQ, 256)

    def attend(query_block):
        scores = jnp.einsum('qhd,khd->hqk', query_block.astype(jnp.float32), all_keys) * QK ** (-0.5)
        scores = scores + lift[:, None, :]
        highest = lax.optimization_barrier(jnp.max(scores, axis=-1, keepdims=True))
        weights = jnp.exp(scores - highest)
        total = lax.optimization_barrier(jnp.sum(weights, axis=-1))
        rounded = lax.optimization_barrier(weights.astype(jnp.bfloat16)).astype(jnp.float32)
        mixed = jnp.einsum('hqk,khd->qhd', rounded, all_values)
        return (mixed / jnp.transpose(total)[:, :, None]).astype(jnp.bfloat16)
    blocks = queries.reshape(SEQ // block, block, HEADS, QK)
    attended = lax.map(attend, blocks).reshape(SEQ, HEADS * HD)
    out = jnp.dot(attended, w_output, preferred_element_type=jnp.float32)
    return (latent_tokens.astype(jnp.float32) + gate_lat * out).astype(jnp.bfloat16)
```

```python
import functools
import math

import jax
import jax.numpy as jnp
from jax import lax
from jax.experimental import pallas as pl
from jax.experimental.pallas import tpu as pltpu
from jax.sharding import PartitionSpec as P

HD = 64
ROPE = 32
QK = 96
KVL = 256
HALF = ROPE // 2
GRID_W = 64
EPS = 1e-06
THETA = 10000.0
LOG2E = math.log2(math.e)
MESH = pl.DeviceIdType.MESH
F32 = jnp.float32
BF16 = jnp.bfloat16
HIGHEST = lax.Precision.HIGHEST
LANES = 128
MSG = 80


def nt_dot(a, b):
    return lax.dot_general(a, b, (((1,), (1,)), ((), ())), preferred_element_type=F32)


def lane_ids(shape):
    return lax.broadcasted_iota(jnp.int32, shape, 1)


def row_ids(shape):
    return lax.broadcasted_iota(jnp.int32, shape, 0)


def silu(v):
    return v / (1.0 + jnp.exp(-v))


def column_tile(row):
    width = row.shape[1]
    full = jnp.concatenate([row, jnp.zeros((1, LANES - width), F32)], axis=1)
    return jnp.broadcast_to(full, (LANES, LANES)).T


def angle_tables(group):
    shape = (HALF, LANES)
    freq_row = row_ids(shape)
    token = lane_ids(shape)
    inverse = jnp.zeros(shape, F32)
    for j in range(HALF // 2):
        inverse = jnp.where(freq_row % (HALF // 2) == j, THETA ** (-j / (HALF // 2)), inverse)
    row = (group * (LANES // GRID_W) + token // GRID_W).astype(F32)
    col = (token % GRID_W).astype(F32)
    angle = jnp.where(freq_row < HALF // 2, row, col) * inverse
    return jnp.cos(angle), jnp.sin(angle)


def rotated(tail, cosine, sine):
    front, back = tail[:HALF], tail[HALF:]
    return jnp.concatenate([front * cosine - back * sine, back * cosine + front * sine], axis=0)


def kernel(
    nz,
    ny,
    ntp,
    tok_h,
    ctx_h,
    cond_h,
    cctx_h,
    mshift_h,
    mscale_h,
    mgate_h,
    ngain_h,
    wq_h,
    qgain_h,
    wdown_h,
    wrope_h,
    kvgain_h,
    wup_h,
    kgain_h,
    lift_s,
    wout_h,
    out_ref,
    gtok,
    ctok,
    cond_v,
    cctx_v,
    mods,
    ngain,
    wq,
    qgain,
    wdown,
    wrope,
    kvgain,
    wup,
    kgain,
    wout,
    zbuf,
    ybuf,
    tbuf,
    nv,
    nvc,
    hid,
    wupt,
    ctab,
    stab,
    msg,
    qbuf,
    qfull,
    keys,
    vals,
    ctxl,
    ctxr,
    ostage,
    obuf,
    rstage,
    rbuf,
    load_sem,
    send_sem,
    recv_sem,
    fwd_send,
    fwd_recv,
):
    sp = lax.axis_index("sp")
    tp = lax.axis_index("tp")
    zi, yi = sp // ny, sp % ny
    core = tp % 2
    rows = tok_h.shape[0]
    width = tok_h.shape[1]
    piece = mods.shape[2]
    crow = ctx_h.shape[0]
    nlat = nz * LANES

    def z_peer(k):
        return (((zi + k) % nz) * ny + yi, tp)

    def y_peer(k):
        return (zi * ny + (yi + k) % ny, tp)

    def t_peer(k):
        return (sp, (tp + k) % ntp)

    sibling = (sp, tp + 1 - 2 * core)

    pairs = [
        (cond_h, cond_v),
        (cctx_h, cctx_v),
        (mshift_h, mods.at[0]),
        (mscale_h, mods.at[1]),
        (mgate_h, mods.at[2]),
        (tok_h, gtok.at[tp]),
        (ctx_h, ctok),
        (ngain_h, ngain),
        (wup_h, wup),
        (kgain_h, kgain),
        (qgain_h, qgain),
        (kvgain_h, kvgain),
        (wdown_h, wdown),
        (wrope_h, wrope),
        (wq_h, wq),
        (wout_h, wout),
    ]
    loads = [pltpu.make_async_copy(a, b, load_sem.at[i]) for i, (a, b) in enumerate(pairs)]
    for copy in loads:
        copy.start()

    barrier = pltpu.get_barrier_semaphore()
    peers = (
        [z_peer(k) for k in range(1, nz)]
        + [y_peer(k) for k in range(1, ny)]
        + [t_peer(k) for k in range(1, ntp)]
    )
    for peer in peers:
        pl.semaphore_signal(barrier, inc=1, device_id=peer, device_id_type=MESH)

    for i in range(5):
        loads[i].wait()
    mod_rows = mods.shape[1]
    fold = LANES // mod_rows
    quarter = sp % fold
    own_row = sp // fold
    lat_row = silu(cond_v[pl.ds(own_row, 1), :])
    ctx_row = silu(cctx_v[pl.ds(own_row, 1), :])
    mine = lane_ids((1, LANES)) // mod_rows == quarter
    signal = jnp.concatenate(
        [jnp.where(mine, lat_row, 0.0), jnp.where(mine, ctx_row, 0.0), jnp.zeros((6, LANES), F32)],
        axis=0,
    )
    block = jnp.concatenate([mods[0], mods[1], mods[2]], axis=1).astype(F32)
    block = jnp.concatenate([block] * fold, axis=0)
    share = jnp.dot(signal, block, precision=HIGHEST, preferred_element_type=F32)
    zbuf[0] = share[0:2]

    pl.semaphore_wait(barrier, len(peers))

    def exchange(src, buf, count, peer, first):
        copies = []
        for k in range(1, count):
            copies.append(
                pltpu.make_async_remote_copy(
                    src_ref=src,
                    dst_ref=buf.at[k],
                    send_sem=send_sem.at[first + k],
                    recv_sem=recv_sem.at[first + k],
                    device_id=peer(k),
                    device_id_type=MESH,
                )
            )
        for copy in copies:
            copy.start()
        return copies

    z_copies = exchange(zbuf.at[0], zbuf, nz, z_peer, 0)

    loads[5].wait()
    tok_copies = []
    for k in range(1, ntp):
        tok_copies.append(
            pltpu.make_async_remote_copy(
                src_ref=gtok.at[tp],
                dst_ref=gtok.at[tp],
                send_sem=send_sem.at[8 + k],
                recv_sem=recv_sem.at[8 + k],
                device_id=t_peer(k),
                device_id_type=MESH,
            )
        )
    for copy in tok_copies:
        copy.start()

    for i in range(6, 12):
        loads[i].wait()
    gain_row = ngain[...]
    cv = ctok[...].astype(F32)
    nvc[...] = cv * lax.rsqrt(jnp.mean(cv * cv, axis=1, keepdims=True) + EPS) * gain_row
    wupt[...] = wup[0].astype(F32).T.astype(BF16)
    keys[...] = jnp.zeros(keys.shape, BF16)
    vals[:, nlat:, :] = jnp.zeros((2, LANES, LANES), BF16)
    ctxl[...] = jnp.zeros(ctxl.shape, F32)
    ctxr[...] = jnp.zeros(ctxr.shape, F32)
    msg[0, :, 64:80, :] = jnp.zeros((2, 16, KVL), BF16)
    hid[LANES:, :] = jnp.zeros((hid.shape[0] - LANES, width), BF16)
    kg = column_tile(kgain[...])
    qg = column_tile(qgain[...]) * (LOG2E * QK ** (-0.5))
    for k in range(nz):
        cosine, sine = angle_tables(((zi + nz - k) % nz) * ny + yi)
        ctab[k] = cosine
        stab[k] = sine

    for copy in z_copies:
        copy.wait_recv()
    total = zbuf[0]
    for k in range(1, nz):
        total = total + zbuf[k]
    ybuf[0] = total
    y_copies = exchange(ybuf.at[0], ybuf, ny, y_peer, 16)

    for copy in tok_copies:
        copy.wait_recv()

    def norm_rows(i, carry):
        v = gtok[i].astype(F32)
        scaled = v * lax.rsqrt(jnp.mean(v * v, axis=1, keepdims=True) + EPS) * gain_row
        nv[pl.ds(pl.multiple_of(i * rows, rows), rows), :] = scaled
        return carry

    lax.fori_loop(0, ntp, norm_rows, 0)

    for copy in y_copies:
        copy.wait_recv()
    total = ybuf[0]
    for k in range(1, ny):
        total = total + ybuf[k]
    tbuf[tp] = total
    t_copies = []
    for k in range(1, ntp):
        t_copies.append(
            pltpu.make_async_remote_copy(
                src_ref=tbuf.at[tp],
                dst_ref=tbuf.at[tp],
                send_sem=send_sem.at[24 + k],
                recv_sem=recv_sem.at[24 + k],
                device_id=t_peer(k),
                device_id_type=MESH,
            )
        )
    for copy in t_copies:
        copy.start()
    for i in range(12, 16):
        loads[i].wait()
    for copy in t_copies:
        copy.wait_recv()

    def vector(which, who):
        return jnp.concatenate(
            [tbuf[t][who : who + 1, which * piece : (which + 1) * piece] for t in range(ntp)],
            axis=1,
        )

    shift_row = vector(0, 0)
    scale_row = 1.0 + vector(1, 0)

    def modulate(i, carry):
        at = pl.ds(pl.multiple_of(i * 16, 16), 16)
        hid[at, :] = (nv[at, :] * scale_row + shift_row).astype(BF16)
        return carry

    lax.fori_loop(0, LANES // 16, modulate, 0)
    ctx_hidden = nvc[...] * (1.0 + vector(1, 1)) + vector(0, 1)
    hid[LANES : LANES + 16, :] = jnp.concatenate(
        [ctx_hidden, jnp.zeros((16 - crow, width), F32)], axis=0
    ).astype(BF16)

    raw = jnp.dot(hid[...], wdown[...], preferred_element_type=F32)
    lat = raw * lax.rsqrt(jnp.mean(raw * raw, axis=1, keepdims=True) + EPS) * kvgain[...]
    rope = jnp.dot(hid[...], wrope[...], preferred_element_type=F32)
    rope = jnp.concatenate([rope, jnp.zeros((hid.shape[0], LANES - ROPE), F32)], axis=1)
    rope_t = rope[:LANES].T[:ROPE]
    ctx_lat = lat[LANES : LANES + crow]
    msg[0, 0, 0:64, :] = lat[0:64].astype(BF16)
    msg[0, 1, 0:64, :] = lat[64:128].astype(BF16)
    msg[0, 0, 64:80, 0:LANES] = rope_t[:16].astype(BF16)
    msg[0, 1, 64:80, 0:LANES] = rope_t[16:].astype(BF16)
    msg[0, 0, 64:80, LANES:] = jnp.concatenate([ctx_lat[:, :LANES], ctx_lat[:, LANES:]], axis=0).astype(BF16)
    msg[0, 1, 64:80, LANES:] = rope[LANES : LANES + 16].astype(BF16)
    k_copies = []
    for k in range(1, nz):
        k_copies.append(
            pltpu.make_async_remote_copy(
                src_ref=msg.at[0, core],
                dst_ref=msg.at[k, core],
                send_sem=send_sem.at[32 + k],
                recv_sem=recv_sem.at[32 + k],
                device_id=z_peer(k),
                device_id_type=MESH,
            )
        )
    for copy in k_copies:
        copy.start()

    raw = jnp.dot(hid[:LANES, :], wq[...], preferred_element_type=F32)
    raw_t = jnp.concatenate([raw, jnp.zeros((LANES, 2 * LANES - 2 * QK), F32)], axis=1).T
    plains, tails = [], []
    for h in range(2):
        u = raw_t[h * QK : (h + 1) * QK]
        inv = lax.rsqrt(jnp.sum(u * u, axis=0, keepdims=True) * (1.0 / QK) + EPS)
        u = u * inv * qg[:QK]
        plains.append(u[:HD])
        tails.append(rotated(u[HD:], ctab[0], stab[0]))
    plain = jnp.concatenate(plains, axis=0).T
    tail = jnp.concatenate(tails, axis=0)
    tail = jnp.concatenate([tail, pltpu.roll(tail, LANES // 2, 1)], axis=0).T
    qbuf[0, 0:LANES, :] = plain.astype(BF16)
    qbuf[0, LANES:, :] = tail[: LANES // 2].astype(BF16)
    q_copies = exchange(qbuf.at[0], qbuf, ny, y_peer, 40)

    def expand_slot(k):
        latent = msg[k, :, 0:64, :].reshape(LANES, KVL)
        rope_k = jnp.concatenate([msg[k, 0, 64:80, 0:LANES], msg[k, 1, 64:80, 0:LANES]], axis=0).astype(F32)
        up = nt_dot(wupt[...], latent)
        shared = jnp.sum(rope_k * rope_k, axis=0, keepdims=True)
        at = pl.ds(k * LANES, LANES)
        for h in range(2):
            part = up[h * HD : (h + 1) * HD]
            inv = lax.rsqrt((jnp.sum(part * part, axis=0, keepdims=True) + shared) * (1.0 / QK) + EPS)
            keys[h, h * HD : (h + 1) * HD, at] = (part * inv * kg[:HD]).astype(BF16)
            turned = rotated(rope_k * inv * kg[HD:QK], ctab[k], stab[k])
            keys[h, LANES + h * ROPE : LANES + (h + 1) * ROPE, at] = turned.astype(BF16)
        value = jnp.dot(latent, wup[1], preferred_element_type=F32)
        low = lane_ids((LANES, LANES)) < HD
        vals[0, at, :] = jnp.where(low, value, 1.0).astype(BF16)
        vals[1, at, :] = jnp.where(low, 1.0, value).astype(BF16)
        ctx_two = msg[k, 0, 64:80, LANES:].astype(F32)
        ctxl[k * crow : (k + 1) * crow, :] = jnp.concatenate([ctx_two[:crow], ctx_two[8 : 8 + crow]], axis=1)
        ctxr[k * crow : (k + 1) * crow, :] = msg[k, 1, 64:80, LANES:].astype(F32)[:crow]

    expand_slot(0)
    forwards = []
    for k in range(1, nz):
        k_copies[k - 1].wait_recv()
        forward = pltpu.make_async_remote_copy(
            src_ref=msg.at[k, core],
            dst_ref=msg.at[k, core],
            send_sem=fwd_send.at[k],
            recv_sem=fwd_recv.at[k],
            device_id=sibling,
            device_id_type=MESH,
        )
        forward.start()
        forwards.append(forward)
        if k > 1:
            forwards[k - 2].wait_recv()
            expand_slot(k - 1)
    forwards[nz - 2].wait_recv()
    expand_slot(nz - 1)

    latent = ctxl[...].astype(BF16)
    rope_k = ctxr[...].T[:ROPE]
    up = nt_dot(wupt[...], latent)
    shared = jnp.sum(rope_k * rope_k, axis=0, keepdims=True)
    at = pl.ds(nlat, LANES)
    for h in range(2):
        part = up[h * HD : (h + 1) * HD]
        inv = lax.rsqrt((jnp.sum(part * part, axis=0, keepdims=True) + shared) * (1.0 / QK) + EPS)
        keys[h, h * HD : (h + 1) * HD, at] = (part * inv * kg[:HD]).astype(BF16)
        keys[h, LANES + h * ROPE : LANES + (h + 1) * ROPE, at] = (rope_k * inv * kg[HD:QK]).astype(BF16)
    value = jnp.dot(latent, wup[1], preferred_element_type=F32)
    low = lane_ids((LANES, LANES)) < HD
    real = row_ids((LANES, LANES)) < nz * crow
    ones = jnp.where(real, 1.0, 0.0)
    vals[0, at, :] = jnp.where(low, value, ones).astype(BF16)
    vals[1, at, :] = jnp.where(low, ones, value).astype(BF16)

    for copy in q_copies:
        copy.wait_recv()
    lifts = [lift_s[0, h] * LOG2E for h in range(2)]
    diagonal = lane_ids((LANES, LANES)) % HD == row_ids((LANES, LANES)) % HD

    def attend(j, carry):
        tails = qbuf[j, LANES:, :]
        turned_tails = pltpu.roll(tails.astype(F32), LANES // 2, 1).astype(BF16)
        q = jnp.concatenate([qbuf[j, 0:LANES, :], jnp.concatenate([tails, turned_tails], axis=0)], axis=1)
        outs = []
        for h in range(2):
            acc = jnp.zeros((LANES, LANES), F32)
            for start in range(0, nlat + LANES, 256):
                size = min(256, nlat + LANES - start)
                s = jnp.dot(q, keys[h, :, start : start + size], preferred_element_type=F32)
                if start < nlat:
                    s = s - lifts[h]
                p = jnp.exp2(s).astype(BF16)
                acc = acc + jnp.dot(p, vals[h, start : start + size, :], preferred_element_type=F32)
            outs.append(acc)
        low = lane_ids((LANES, LANES)) < HD
        num = jnp.where(low, outs[0], outs[1])
        den = jnp.where(low, outs[1], outs[0])
        den = jnp.where(diagonal, den, 0.0)
        packed = jnp.concatenate(
            [
                jnp.sum(den[:HD], axis=0, keepdims=True),
                jnp.sum(den[HD:], axis=0, keepdims=True),
            ],
            axis=0,
        )
        hi = packed.astype(BF16).astype(F32)
        lo = packed - hi
        ostage[j, 0:LANES, :] = num.astype(BF16)
        ostage[j, LANES:, :] = jnp.concatenate([hi, lo, jnp.zeros((12, LANES), F32)], axis=0).astype(BF16)
        return carry

    o_copies = []
    for j in [k for k in range(1, ny)] + [0]:
        attend(j, 0)
        if j:
            copy = pltpu.make_async_remote_copy(
                src_ref=ostage.at[j],
                dst_ref=obuf.at[j],
                send_sem=send_sem.at[48 + j],
                recv_sem=recv_sem.at[48 + j],
                device_id=y_peer(ny - j),
                device_id_type=MESH,
            )
            copy.start()
            o_copies.append(copy)
    for copy in o_copies:
        copy.wait_recv()
    num = ostage[0, 0:LANES, :].astype(F32)
    den = ostage[0, LANES:, :].astype(F32)
    for j in range(1, ny):
        num = num + obuf[j, 0:LANES, :].astype(F32)
        den = den + obuf[j, LANES:, :].astype(F32)
    den = den[0:2] + den[2:4]
    spread = jnp.concatenate(
        [
            jnp.broadcast_to(den[0:1], (HD, LANES)),
            jnp.broadcast_to(den[1:2], (HD, LANES)),
        ],
        axis=0,
    )
    spread = jnp.where(diagonal, spread, 0.0)
    swap = jnp.where((lane_ids((LANES, LANES)) < HD) != (row_ids((LANES, LANES)) < HD), 1.0, 0.0)
    spread = jnp.dot(spread, swap, precision=HIGHEST, preferred_element_type=F32)
    attended = (num / spread).astype(BF16)

    proj = jnp.dot(attended, wout[...], preferred_element_type=F32).astype(BF16)
    for t in range(ntp):
        rstage[t] = proj[t * rows : (t + 1) * rows]
    r_copies = []
    for k in range(1, ntp):
        r_copies.append(
            pltpu.make_async_remote_copy(
                src_ref=rstage.at[(tp + k) % ntp],
                dst_ref=rbuf.at[k],
                send_sem=send_sem.at[56 + k],
                recv_sem=recv_sem.at[56 + k],
                device_id=t_peer(k),
                device_id_type=MESH,
            )
        )
    for copy in r_copies:
        copy.start()
    result = rstage[tp].astype(F32)
    for copy in r_copies:
        copy.wait_recv()
    for k in range(1, ntp):
        result = result + rbuf[k].astype(F32)
    out_ref[...] = (gtok[tp].astype(F32) + vector(2, 0) * result).astype(BF16)

    for copy in z_copies + tok_copies + y_copies + t_copies + k_copies + q_copies + forwards + o_copies + r_copies:
        copy.wait_send()


def solution(mesh, nz=8):
    nsp, ntp = mesh.shape["sp"], mesh.shape["tp"]
    ny = nsp // nz

    def local(
        latent_tokens,
        context_tokens,
        cond,
        ctx_cond,
        mod_shift,
        mod_scale,
        mod_gate,
        norm_gain,
        w_query,
        query_gain,
        w_down_kv,
        w_rope_key,
        kv_gain,
        w_up_kv,
        key_gain,
        ctx_lift,
        w_output,
    ):
        rows, width = latent_tokens.shape
        crow = context_tokens.shape[0]
        piece = mod_shift.shape[1]
        lat = nz * LANES
        vm = pltpu.VMEM
        anywhere = pl.BlockSpec(memory_space=pl.ANY)
        smem = pl.BlockSpec(memory_space=pltpu.SMEM)
        return pl.pallas_call(
            functools.partial(kernel, nz, ny, ntp),
            out_shape=jax.ShapeDtypeStruct((rows, width), BF16),
            in_specs=[anywhere] * 15 + [smem, anywhere],
            out_specs=pl.BlockSpec(memory_space=pltpu.VMEM),
            scratch_shapes=[
                vm((ntp, rows, width), BF16),
                vm((crow, width), BF16),
                vm((width // LANES, LANES), F32),
                vm((width // LANES, LANES), F32),
                vm((3, mod_shift.shape[0], piece), BF16),
                vm((1, width), F32),
                vm(w_query.shape, BF16),
                vm((1, QK), F32),
                vm(w_down_kv.shape, BF16),
                vm(w_rope_key.shape, BF16),
                vm((1, KVL), F32),
                vm(w_up_kv.shape, BF16),
                vm((1, QK), F32),
                vm(w_output.shape, BF16),
                vm((nz, 2, 3 * piece), F32),
                vm((ny, 2, 3 * piece), F32),
                vm((ntp, 2, 3 * piece), F32),
                vm((LANES, width), F32),
                vm((crow, width), F32),
                vm((LANES + 16, width), BF16),
                vm((LANES, KVL), BF16),
                vm((nz, HALF, LANES), F32),
                vm((nz, HALF, LANES), F32),
                vm((nz, 2, MSG, KVL), BF16),
                vm((ny, LANES + HD, LANES), BF16),
                vm((8, LANES), F32),
                vm((2, 2 * LANES, lat + LANES), BF16),
                vm((2, lat + LANES, LANES), BF16),
                vm((LANES, KVL), F32),
                vm((LANES, LANES), F32),
                vm((ny, LANES + 16, LANES), BF16),
                vm((ny, LANES + 16, LANES), BF16),
                vm((ntp, rows, width), BF16),
                vm((ntp, rows, width), BF16),
                pltpu.SemaphoreType.DMA((16,)),
                pltpu.SemaphoreType.DMA((64,)),
                pltpu.SemaphoreType.DMA((64,)),
                pltpu.SemaphoreType.DMA((8,)),
                pltpu.SemaphoreType.DMA((8,)),
            ],
            compiler_params=pltpu.CompilerParams(
                collective_id=0, has_side_effects=True, vmem_limit_bytes=60 * 1024 * 1024
            ),
        )(
            latent_tokens,
            context_tokens,
            cond.reshape(width // LANES, LANES),
            ctx_cond.reshape(width // LANES, LANES),
            mod_shift,
            mod_scale,
            mod_gate,
            norm_gain.reshape(1, width),
            w_query,
            query_gain.reshape(1, QK),
            w_down_kv,
            w_rope_key,
            kv_gain.reshape(1, KVL),
            w_up_kv,
            key_gain.reshape(1, QK),
            ctx_lift.reshape(1, 2),
            w_output,
        )

    in_specs = (
        P(("sp", "tp"), None),
        P("sp", None),
        P(),
        P(),
        P("sp", "tp"),
        P("sp", "tp"),
        P("sp", "tp"),
        P(),
        P(None, "tp"),
        P(),
        P(),
        P(),
        P(),
        P(None, None, "tp"),
        P(),
        P("tp"),
        P("tp", None),
    )
    return jax.shard_map(local, mesh=mesh, in_specs=in_specs, out_specs=P(("sp", "tp"), None), check_vma=False)
```

```python
import functools
import math

import jax
import jax.numpy as jnp
from jax import lax
from jax.experimental import pallas as pl
from jax.experimental.pallas import tpu as pltpu
from jax.sharding import PartitionSpec as P

HD = 64
ROPE = 32
QK = 96
KVL = 256
HALF = ROPE // 2
GRID_W = 64
EPS = 1e-06
THETA = 10000.0
LOG2E = math.log2(math.e)
MESH = pl.DeviceIdType.MESH
F32 = jnp.float32
BF16 = jnp.bfloat16
HIGHEST = lax.Precision.HIGHEST
LANES = 128
MSG = 80


def nt_dot(a, b):
    return lax.dot_general(a, b, (((1,), (1,)), ((), ())), preferred_element_type=F32)


def lane_ids(shape):
    return lax.broadcasted_iota(jnp.int32, shape, 1)


def row_ids(shape):
    return lax.broadcasted_iota(jnp.int32, shape, 0)


def silu(v):
    return v / (1.0 + jnp.exp(-v))


def column_tile(row):
    width = row.shape[1]
    full = jnp.concatenate([row, jnp.zeros((1, LANES - width), F32)], axis=1)
    return jnp.broadcast_to(full, (LANES, LANES)).T


def angle_tables(group):
    shape = (HALF, LANES)
    freq_row = row_ids(shape)
    token = lane_ids(shape)
    inverse = jnp.zeros(shape, F32)
    for j in range(HALF // 2):
        inverse = jnp.where(freq_row % (HALF // 2) == j, THETA ** (-j / (HALF // 2)), inverse)
    row = (group * (LANES // GRID_W) + token // GRID_W).astype(F32)
    col = (token % GRID_W).astype(F32)
    angle = jnp.where(freq_row < HALF // 2, row, col) * inverse
    return jnp.cos(angle), jnp.sin(angle)


def rotated(tail, cosine, sine):
    front, back = tail[:HALF], tail[HALF:]
    return jnp.concatenate([front * cosine - back * sine, back * cosine + front * sine], axis=0)


def kernel(
    nz,
    ny,
    ntp,
    tok_h,
    ctx_h,
    cond_h,
    cctx_h,
    mshift_h,
    mscale_h,
    mgate_h,
    ngain_h,
    wq_h,
    qgain_h,
    wdown_h,
    wrope_h,
    kvgain_h,
    wup_h,
    kgain_h,
    lift_s,
    wout_h,
    out_ref,
    gtok,
    ctok,
    cond_v,
    cctx_v,
    mods,
    ngain,
    wq,
    qgain,
    wdown,
    wrope,
    kvgain,
    wup,
    kgain,
    wout,
    zbuf,
    ybuf,
    tbuf,
    gzbuf,
    gybuf,
    gtbuf,
    nv,
    nvc,
    hid,
    wupt,
    ctab,
    stab,
    msg,
    qbuf,
    keys,
    vals,
    ctxl,
    ctxr,
    ostage,
    obuf,
    rstage,
    rbuf,
    load_sem,
    send_sem,
    recv_sem,
    fwd_send,
    fwd_recv,
):
    sp = lax.axis_index("sp")
    tp = lax.axis_index("tp")
    zi, yi = sp // ny, sp % ny
    core = tp % 2
    rows = tok_h.shape[0]
    width = tok_h.shape[1]
    piece = mods.shape[2]
    crow = ctx_h.shape[0]
    nlat = nz * LANES

    def z_peer(k):
        return (((zi + k) % nz) * ny + yi, tp)

    def y_peer(k):
        return (zi * ny + (yi + k) % ny, tp)

    def t_peer(k):
        return (sp, (tp + k) % ntp)

    sibling = (sp, tp + 1 - 2 * core)

    pairs = [
        (cond_h, cond_v),
        (cctx_h, cctx_v),
        (mshift_h, mods.at[0]),
        (mscale_h, mods.at[1]),
        (mgate_h, mods.at[2]),
        (tok_h, gtok.at[tp]),
        (ctx_h, ctok),
        (ngain_h, ngain),
        (wup_h, wup),
        (kgain_h, kgain),
        (qgain_h, qgain),
        (kvgain_h, kvgain),
        (wdown_h, wdown),
        (wrope_h, wrope),
        (wq_h, wq),
        (wout_h, wout),
    ]
    loads = [pltpu.make_async_copy(a, b, load_sem.at[i]) for i, (a, b) in enumerate(pairs)]
    for copy in loads:
        copy.start()

    barrier = pltpu.get_barrier_semaphore()
    peers = (
        [z_peer(k) for k in range(1, nz)]
        + [y_peer(k) for k in range(1, ny)]
        + [t_peer(k) for k in range(1, ntp)]
    )
    for peer in peers:
        pl.semaphore_signal(barrier, inc=1, device_id=peer, device_id_type=MESH)

    for i in range(5):
        loads[i].wait()
    mod_rows = mods.shape[1]
    fold = LANES // mod_rows
    quarter = sp % fold
    own_row = sp // fold
    lat_row = silu(cond_v[pl.ds(own_row, 1), :])
    ctx_row = silu(cctx_v[pl.ds(own_row, 1), :])
    mine = lane_ids((1, LANES)) // mod_rows == quarter
    signal = jnp.concatenate(
        [jnp.where(mine, lat_row, 0.0), jnp.where(mine, ctx_row, 0.0), jnp.zeros((6, LANES), F32)],
        axis=0,
    )
    block = jnp.concatenate([mods[0], mods[1], mods[2]], axis=1).astype(F32)
    block = jnp.concatenate([block] * fold, axis=0)
    share = jnp.dot(signal, block, precision=HIGHEST, preferred_element_type=F32)
    zbuf[0] = share[0:2, : 2 * piece]
    gzbuf[0] = share[0:1, 2 * piece :]

    for i in range(6, 12):
        loads[i].wait()
    gain_row = ngain[...]
    cv = ctok[...].astype(F32)
    nvc[...] = cv * lax.rsqrt(jnp.mean(cv * cv, axis=1, keepdims=True) + EPS) * gain_row
    wupt[...] = wup[0].astype(F32).T.astype(BF16)
    keys[...] = jnp.zeros(keys.shape, BF16)
    vals[:, nlat:, :] = jnp.zeros((2, LANES, LANES), BF16)
    ctxl[...] = jnp.zeros(ctxl.shape, F32)
    ctxr[...] = jnp.zeros(ctxr.shape, F32)
    msg[0, :, 64:80, :] = jnp.zeros((2, 16, KVL), BF16)
    hid[LANES:, :] = jnp.zeros((hid.shape[0] - LANES, width), BF16)
    kg = column_tile(kgain[...])
    qg = column_tile(qgain[...]) * (LOG2E * QK ** (-0.5))
    for k in range(nz):
        cosine, sine = angle_tables(((zi + nz - k) % nz) * ny + yi)
        ctab[k] = cosine
        stab[k] = sine


    pl.semaphore_wait(barrier, len(peers))

    def near_first(count):
        return sorted(range(1, count), key=lambda k: min(k, count - k))

    def exchange(src, buf, count, peer, first, near=False):
        copies = []
        for k in range(1, count):
            copies.append(
                pltpu.make_async_remote_copy(
                    src_ref=src,
                    dst_ref=buf.at[k],
                    send_sem=send_sem.at[first + k],
                    recv_sem=recv_sem.at[first + k],
                    device_id=peer(k),
                    device_id_type=MESH,
                )
            )
        order = near_first(count)
        for k in order if near else order[::-1]:
            copies[k - 1].start()
        return copies

    z_copies = exchange(zbuf.at[0], zbuf, nz, z_peer, 0)
    gz_copies = exchange(gzbuf.at[0], gzbuf, nz, z_peer, 64)

    loads[5].wait()
    tok_copies = []
    for k in range(1, ntp):
        tok_copies.append(
            pltpu.make_async_remote_copy(
                src_ref=gtok.at[tp],
                dst_ref=gtok.at[tp],
                send_sem=send_sem.at[8 + k],
                recv_sem=recv_sem.at[8 + k],
                device_id=t_peer(k),
                device_id_type=MESH,
            )
        )
    for copy in tok_copies:
        copy.start()

    for copy in z_copies:
        copy.wait_recv()
    total = zbuf[0]
    for k in range(1, nz):
        total = total + zbuf[k]
    ybuf[0] = total
    y_copies = exchange(ybuf.at[0], ybuf, ny, y_peer, 16)
    for copy in gz_copies:
        copy.wait_recv()
    total = gzbuf[0]
    for k in range(1, nz):
        total = total + gzbuf[k]
    gybuf[0] = total
    gy_copies = exchange(gybuf.at[0], gybuf, ny, y_peer, 72)

    for copy in tok_copies:
        copy.wait_recv()

    def norm_rows(i, carry):
        v = gtok[i].astype(F32)
        scaled = v * lax.rsqrt(jnp.mean(v * v, axis=1, keepdims=True) + EPS) * gain_row
        nv[pl.ds(pl.multiple_of(i * rows, rows), rows), :] = scaled
        return carry

    lax.fori_loop(0, ntp, norm_rows, 0)

    for copy in y_copies:
        copy.wait_recv()
    total = ybuf[0]
    for k in range(1, ny):
        total = total + ybuf[k]
    tbuf[tp] = total

    def spread_tp(buf, first):
        copies = []
        for k in range(1, ntp):
            copies.append(
                pltpu.make_async_remote_copy(
                    src_ref=buf.at[tp],
                    dst_ref=buf.at[tp],
                    send_sem=send_sem.at[first + k],
                    recv_sem=recv_sem.at[first + k],
                    device_id=t_peer(k),
                    device_id_type=MESH,
                )
            )
        for copy in copies:
            copy.start()
        return copies

    t_copies = spread_tp(tbuf, 24)
    for copy in gy_copies:
        copy.wait_recv()
    total = gybuf[0]
    for k in range(1, ny):
        total = total + gybuf[k]
    gtbuf[tp] = total
    gt_copies = spread_tp(gtbuf, 80)
    for i in range(12, 16):
        loads[i].wait()
    for copy in t_copies:
        copy.wait_recv()

    def vector(which, who):
        return jnp.concatenate(
            [tbuf[t][who : who + 1, which * piece : (which + 1) * piece] for t in range(ntp)],
            axis=1,
        )

    shift_row = vector(0, 0)
    scale_row = 1.0 + vector(1, 0)

    def modulate(i, carry):
        at = pl.ds(pl.multiple_of(i * 16, 16), 16)
        hid[at, :] = (nv[at, :] * scale_row + shift_row).astype(BF16)
        return carry

    lax.fori_loop(0, LANES // 16, modulate, 0)
    ctx_hidden = nvc[...] * (1.0 + vector(1, 1)) + vector(0, 1)
    hid[LANES : LANES + 16, :] = jnp.concatenate(
        [ctx_hidden, jnp.zeros((16 - crow, width), F32)], axis=0
    ).astype(BF16)

    raw = jnp.dot(hid[...], wdown[...], preferred_element_type=F32)
    lat = raw * lax.rsqrt(jnp.mean(raw * raw, axis=1, keepdims=True) + EPS) * kvgain[...]
    rope_t = nt_dot(wrope[...], hid[:LANES, :])
    rope_c = nt_dot(hid[LANES:, :], wrope[...])
    rope_c = jnp.concatenate([rope_c, jnp.zeros((16, LANES - ROPE), F32)], axis=1)
    ctx_lat = lat[LANES : LANES + crow]
    msg[0, 0, 0:64, :] = lat[0:64].astype(BF16)
    msg[0, 1, 0:64, :] = lat[64:128].astype(BF16)
    msg[0, 0, 64:80, 0:LANES] = rope_t[:16].astype(BF16)
    msg[0, 1, 64:80, 0:LANES] = rope_t[16:].astype(BF16)
    msg[0, 0, 64:80, LANES:] = jnp.concatenate([ctx_lat[:, :LANES], ctx_lat[:, LANES:]], axis=0).astype(BF16)
    msg[0, 1, 64:80, LANES:] = rope_c.astype(BF16)
    k_copies = []
    for k in range(1, nz):
        k_copies.append(
            pltpu.make_async_remote_copy(
                src_ref=msg.at[0, core],
                dst_ref=msg.at[k, core],
                send_sem=send_sem.at[32 + k],
                recv_sem=recv_sem.at[32 + k],
                device_id=z_peer(k),
                device_id_type=MESH,
            )
        )
    for k in near_first(nz):
        k_copies[k - 1].start()

    raw_t = nt_dot(wq[...], hid[:LANES, :])
    plains, tails = [], []
    for h in range(2):
        u = raw_t[h * QK : (h + 1) * QK]
        inv = lax.rsqrt(jnp.sum(u * u, axis=0, keepdims=True) * (1.0 / QK) + EPS)
        u = u * inv * qg[:QK]
        plains.append(u[:HD])
        tails.append(rotated(u[HD:], ctab[0], stab[0]))
    plain = jnp.concatenate(plains, axis=0).T
    tail = jnp.concatenate(tails, axis=0)
    tail = jnp.concatenate([tail, pltpu.roll(tail, LANES // 2, 1)], axis=0).T
    qbuf[0, 0:LANES, :] = plain.astype(BF16)
    qbuf[0, LANES:, :] = tail[: LANES // 2].astype(BF16)
    q_copies = exchange(qbuf.at[0], qbuf, ny, y_peer, 40, near=True)

    def expand_slot(k):
        latent = msg[k, :, 0:64, :].reshape(LANES, KVL)
        rope_k = jnp.concatenate([msg[k, 0, 64:80, 0:LANES], msg[k, 1, 64:80, 0:LANES]], axis=0).astype(F32)
        up = nt_dot(wupt[...], latent)
        shared = jnp.sum(rope_k * rope_k, axis=0, keepdims=True)
        at = pl.ds(k * LANES, LANES)
        for h in range(2):
            part = up[h * HD : (h + 1) * HD]
            inv = lax.rsqrt((jnp.sum(part * part, axis=0, keepdims=True) + shared) * (1.0 / QK) + EPS)
            keys[h, h * HD : (h + 1) * HD, at] = (part * inv * kg[:HD]).astype(BF16)
            turned = rotated(rope_k * inv * kg[HD:QK], ctab[k], stab[k])
            keys[h, LANES + h * ROPE : LANES + (h + 1) * ROPE, at] = turned.astype(BF16)
        value = jnp.dot(latent, wup[1], preferred_element_type=F32)
        low = lane_ids((LANES, LANES)) < HD
        vals[0, at, :] = jnp.where(low, value, 1.0).astype(BF16)
        vals[1, at, :] = jnp.where(low, 1.0, value).astype(BF16)
        ctx_two = msg[k, 0, 64:80, LANES:].astype(F32)
        ctxl[k * crow : (k + 1) * crow, :] = jnp.concatenate([ctx_two[:crow], ctx_two[8 : 8 + crow]], axis=1)
        ctxr[k * crow : (k + 1) * crow, :] = msg[k, 1, 64:80, LANES:].astype(F32)[:crow]

    expand_slot(0)
    forwards = []
    passed = []
    for k in near_first(nz):
        k_copies[k - 1].wait_recv()
        forward = pltpu.make_async_remote_copy(
            src_ref=msg.at[k, core],
            dst_ref=msg.at[k, core],
            send_sem=fwd_send.at[k],
            recv_sem=fwd_recv.at[k],
            device_id=sibling,
            device_id_type=MESH,
        )
        forward.start()
        forwards.append(forward)
        passed.append(k)
        if len(passed) > 1:
            forwards[-2].wait_recv()
            expand_slot(passed[-2])
    forwards[-1].wait_recv()
    expand_slot(passed[-1])

    latent = ctxl[...].astype(BF16)
    rope_k = ctxr[...].T[:ROPE]
    up = nt_dot(wupt[...], latent)
    shared = jnp.sum(rope_k * rope_k, axis=0, keepdims=True)
    at = pl.ds(nlat, LANES)
    for h in range(2):
        part = up[h * HD : (h + 1) * HD]
        inv = lax.rsqrt((jnp.sum(part * part, axis=0, keepdims=True) + shared) * (1.0 / QK) + EPS)
        keys[h, h * HD : (h + 1) * HD, at] = (part * inv * kg[:HD]).astype(BF16)
        keys[h, LANES + h * ROPE : LANES + (h + 1) * ROPE, at] = (rope_k * inv * kg[HD:QK]).astype(BF16)
    value = jnp.dot(latent, wup[1], preferred_element_type=F32)
    low = lane_ids((LANES, LANES)) < HD
    real = row_ids((LANES, LANES)) < nz * crow
    ones = jnp.where(real, 1.0, 0.0)
    vals[0, at, :] = jnp.where(low, value, ones).astype(BF16)
    vals[1, at, :] = jnp.where(low, ones, value).astype(BF16)

    diagonal = lane_ids((LANES, LANES)) % HD == row_ids((LANES, LANES)) % HD

    low = lane_ids((LANES, LANES)) < HD
    late = lane_ids((1, nlat + LANES)) < nlat
    lifts = [jnp.where(late, lift_s[0, h] * LOG2E, 0.0) for h in range(2)]

    def whole_query(j):
        tails = qbuf[j, LANES:, :]
        turned_tails = pltpu.roll(tails.astype(F32), LANES // 2, 1).astype(BF16)
        return jnp.concatenate([qbuf[j, 0:LANES, :], jnp.concatenate([tails, turned_tails], axis=0)], axis=1)

    def attend(slots):
        q = jnp.concatenate([whole_query(j) for j in slots], axis=0)
        outs = []
        for h in range(2):
            p = jnp.exp2(jnp.dot(q, keys[h], preferred_element_type=F32) - lifts[h]).astype(BF16)
            outs.append(jnp.dot(p, vals[h], preferred_element_type=F32))
        for i, j in enumerate(slots):
            first, second = (out[i * LANES : (i + 1) * LANES] for out in outs)
            den = jnp.where(diagonal, jnp.where(low, second, first), 0.0)
            packed = jnp.concatenate(
                [
                    jnp.sum(den[:HD], axis=0, keepdims=True),
                    jnp.sum(den[HD:], axis=0, keepdims=True),
                ],
                axis=0,
            )
            hi = packed.astype(BF16).astype(F32)
            lo = packed - hi
            ostage[j, 0:LANES, :] = jnp.where(low, first, second).astype(BF16)
            ostage[j, LANES:, :] = jnp.concatenate([hi, lo, jnp.zeros((12, LANES), F32)], axis=0).astype(BF16)

    o_copies = []
    order = sorted(range(ny), key=lambda j: min(j, ny - j))
    for at in range(0, ny, 2):
        slots = order[at : at + 2]
        for j in slots:
            if j:
                q_copies[j - 1].wait_recv()
        attend(slots)
        for j in slots:
            if j == 0:
                continue
            copy = pltpu.make_async_remote_copy(
                src_ref=ostage.at[j],
                dst_ref=obuf.at[j],
                send_sem=send_sem.at[48 + j],
                recv_sem=recv_sem.at[48 + j],
                device_id=y_peer(ny - j),
                device_id_type=MESH,
            )
            copy.start()
            o_copies.append(copy)
    for copy in o_copies:
        copy.wait_recv()
    num = ostage[0, 0:LANES, :].astype(F32)
    den = ostage[0, LANES:, :].astype(F32)
    for j in range(1, ny):
        num = num + obuf[j, 0:LANES, :].astype(F32)
        den = den + obuf[j, LANES:, :].astype(F32)
    den = den[0:2] + den[2:4]
    spread = jnp.concatenate(
        [
            jnp.broadcast_to(den[0:1], (HD, LANES)),
            jnp.broadcast_to(den[1:2], (HD, LANES)),
        ],
        axis=0,
    )
    spread = jnp.where(diagonal, spread, 0.0)
    swap = jnp.where((lane_ids((LANES, LANES)) < HD) != (row_ids((LANES, LANES)) < HD), 1.0, 0.0)
    spread = jnp.dot(spread, swap, precision=HIGHEST, preferred_element_type=F32)
    attended = (num / spread).astype(BF16)

    proj = jnp.dot(attended, wout[...], preferred_element_type=F32).astype(BF16)
    for t in range(ntp):
        rstage[t] = proj[t * rows : (t + 1) * rows]
    r_copies = []
    for k in range(1, ntp):
        r_copies.append(
            pltpu.make_async_remote_copy(
                src_ref=rstage.at[(tp + k) % ntp],
                dst_ref=rbuf.at[k],
                send_sem=send_sem.at[56 + k],
                recv_sem=recv_sem.at[56 + k],
                device_id=t_peer(k),
                device_id_type=MESH,
            )
        )
    for copy in r_copies:
        copy.start()
    result = rstage[tp].astype(F32)
    for copy in r_copies:
        copy.wait_recv()
    for k in range(1, ntp):
        result = result + rbuf[k].astype(F32)
    for copy in gt_copies:
        copy.wait_recv()
    gate_row = jnp.concatenate([gtbuf[t] for t in range(ntp)], axis=1)
    out_ref[...] = (gtok[tp].astype(F32) + gate_row * result).astype(BF16)

    for copy in gz_copies + gy_copies + gt_copies + z_copies + tok_copies + y_copies + t_copies + k_copies + q_copies + forwards + o_copies + r_copies:
        copy.wait_send()


def solution(mesh, nz=8):
    nsp, ntp = mesh.shape["sp"], mesh.shape["tp"]
    ny = nsp // nz

    def local(
        latent_tokens,
        context_tokens,
        cond,
        ctx_cond,
        mod_shift,
        mod_scale,
        mod_gate,
        norm_gain,
        w_query,
        query_gain,
        w_down_kv,
        w_rope_key,
        kv_gain,
        w_up_kv,
        key_gain,
        ctx_lift,
        w_output,
    ):
        rows, width = latent_tokens.shape
        crow = context_tokens.shape[0]
        piece = mod_shift.shape[1]
        lat = nz * LANES
        vm = pltpu.VMEM
        anywhere = pl.BlockSpec(memory_space=pl.ANY)
        smem = pl.BlockSpec(memory_space=pltpu.SMEM)
        return pl.pallas_call(
            functools.partial(kernel, nz, ny, ntp),
            out_shape=jax.ShapeDtypeStruct((rows, width), BF16),
            in_specs=[anywhere] * 15 + [smem, anywhere],
            out_specs=pl.BlockSpec(memory_space=pltpu.VMEM),
            scratch_shapes=[
                vm((ntp, rows, width), BF16),
                vm((crow, width), BF16),
                vm((width // LANES, LANES), F32),
                vm((width // LANES, LANES), F32),
                vm((3, mod_shift.shape[0], piece), BF16),
                vm((1, width), F32),
                vm(w_query.shape[::-1], BF16),
                vm((1, QK), F32),
                vm(w_down_kv.shape, BF16),
                vm(w_rope_key.shape[::-1], BF16),
                vm((1, KVL), F32),
                vm(w_up_kv.shape, BF16),
                vm((1, QK), F32),
                vm(w_output.shape, BF16),
                vm((nz, 2, 2 * piece), F32),
                vm((ny, 2, 2 * piece), F32),
                vm((ntp, 2, 2 * piece), F32),
                vm((nz, 1, piece), F32),
                vm((ny, 1, piece), F32),
                vm((ntp, 1, piece), F32),
                vm((LANES, width), F32),
                vm((crow, width), F32),
                vm((LANES + 16, width), BF16),
                vm((LANES, KVL), BF16),
                vm((nz, HALF, LANES), F32),
                vm((nz, HALF, LANES), F32),
                vm((nz, 2, MSG, KVL), BF16),
                vm((ny, LANES + HD, LANES), BF16),
                vm((2, 2 * LANES, lat + LANES), BF16),
                vm((2, lat + LANES, LANES), BF16),
                vm((LANES, KVL), F32),
                vm((LANES, LANES), F32),
                vm((ny, LANES + 16, LANES), BF16),
                vm((ny, LANES + 16, LANES), BF16),
                vm((ntp, rows, width), BF16),
                vm((ntp, rows, width), BF16),
                pltpu.SemaphoreType.DMA((16,)),
                pltpu.SemaphoreType.DMA((96,)),
                pltpu.SemaphoreType.DMA((96,)),
                pltpu.SemaphoreType.DMA((8,)),
                pltpu.SemaphoreType.DMA((8,)),
            ],
            compiler_params=pltpu.CompilerParams(
                collective_id=0, has_side_effects=True, vmem_limit_bytes=60 * 1024 * 1024
            ),
        )(
            latent_tokens,
            context_tokens,
            cond.reshape(width // LANES, LANES),
            ctx_cond.reshape(width // LANES, LANES),
            mod_shift,
            mod_scale,
            mod_gate,
            norm_gain.reshape(1, width),
            w_query.T,
            query_gain.reshape(1, QK),
            w_down_kv,
            w_rope_key.T,
            kv_gain.reshape(1, KVL),
            w_up_kv,
            key_gain.reshape(1, QK),
            ctx_lift.reshape(1, 2),
            w_output,
        )

    in_specs = (
        P(("sp", "tp"), None),
        P("sp", None),
        P(),
        P(),
        P("sp", "tp"),
        P("sp", "tp"),
        P("sp", "tp"),
        P(),
        P(None, "tp"),
        P(),
        P(),
        P(),
        P(),
        P(None, None, "tp"),
        P(),
        P("tp"),
        P("tp", None),
    )
    return jax.shard_map(local, mesh=mesh, in_specs=in_specs, out_specs=P(("sp", "tp"), None), check_vma=False)
```

```python
import functools
import math

import jax
import jax.numpy as jnp
from jax import lax
from jax.experimental import pallas as pl
from jax.experimental.pallas import tpu as pltpu
from jax.sharding import PartitionSpec as P

HD = 64
ROPE = 32
QK = 96
KVL = 256
HALF = ROPE // 2
GRID_W = 64
EPS = 1e-06
THETA = 10000.0
LOG2E = math.log2(math.e)
MESH = pl.DeviceIdType.MESH
F32 = jnp.float32
BF16 = jnp.bfloat16
HIGHEST = lax.Precision.HIGHEST
LANES = 128
MSG = 80


def nt_dot(a, b):
    return lax.dot_general(a, b, (((1,), (1,)), ((), ())), preferred_element_type=F32)


def lane_ids(shape):
    return lax.broadcasted_iota(jnp.int32, shape, 1)


def row_ids(shape):
    return lax.broadcasted_iota(jnp.int32, shape, 0)


def silu(v):
    return v / (1.0 + jnp.exp(-v))


def column_tile(row):
    width = row.shape[1]
    full = jnp.concatenate([row, jnp.zeros((1, LANES - width), F32)], axis=1)
    return jnp.broadcast_to(full, (LANES, LANES)).T


class Flight:
    def __init__(self, sent, copy):
        self.copy, self.landed = copy, False
        sent.append(self)
        copy.start()

    def wait_recv(self):
        self.landed = True
        self.copy.wait_recv()

    def wait_send(self):
        self.copy.wait_send()


def angle_tables(group):
    shape = (HALF, LANES)
    freq_row = row_ids(shape)
    token = lane_ids(shape)
    inverse = jnp.zeros(shape, F32)
    for j in range(HALF // 2):
        inverse = jnp.where(freq_row % (HALF // 2) == j, THETA ** (-j / (HALF // 2)), inverse)
    row = (group * (LANES // GRID_W) + token // GRID_W).astype(F32)
    col = (token % GRID_W).astype(F32)
    angle = jnp.where(freq_row < HALF // 2, row, col) * inverse
    return jnp.cos(angle), jnp.sin(angle)


def rotated(tail, cosine, sine):
    front, back = tail[:HALF], tail[HALF:]
    return jnp.concatenate([front * cosine - back * sine, back * cosine + front * sine], axis=0)


def kernel(
    nz,
    ny,
    ntp,
    tok_h,
    ctx_h,
    cond_h,
    cctx_h,
    mshift_h,
    mscale_h,
    mgate_h,
    ngain_h,
    wq_h,
    qgain_h,
    wdown_h,
    wrope_h,
    kvgain_h,
    wup_h,
    kgain_h,
    lift_s,
    wout_h,
    out_ref,
    gtok,
    ctok,
    cond_v,
    cctx_v,
    mods,
    ngain,
    wq,
    qgain,
    wdown,
    wrope,
    kvgain,
    wup,
    kgain,
    wout,
    zbuf,
    ybuf,
    tbuf,
    gzbuf,
    gybuf,
    gtbuf,
    nv,
    nvc,
    hid,
    wupt,
    ctab,
    stab,
    msg,
    qbuf,
    keys,
    vals,
    ctxl,
    ctxr,
    ostage,
    obuf,
    opass,
    rstage,
    rbuf,
    load_sem,
    send_sem,
    recv_sem,
):
    sp = lax.axis_index("sp")
    tp = lax.axis_index("tp")
    zi, yi = sp // ny, sp % ny
    core = tp % 2
    rows = tok_h.shape[0]
    width = tok_h.shape[1]
    piece = mods.shape[2]
    crow = ctx_h.shape[0]
    nlat = nz * LANES

    def z_peer(k):
        return (((zi + k) % nz) * ny + yi, tp)

    def y_peer(k):
        return (zi * ny + (yi + k) % ny, tp)

    def t_peer(k):
        return (sp, (tp + k) % ntp)

    sibling = (sp, tp + 1 - 2 * core)

    def x_index(k):
        return (tp + 2 * k) % ntp

    def x_peer(k):
        return (sp, x_index(k))

    pairs = [
        (cond_h, cond_v),
        (cctx_h, cctx_v),
        (mshift_h, mods.at[0]),
        (mscale_h, mods.at[1]),
        (mgate_h, mods.at[2]),
        (tok_h, gtok.at[tp]),
        (ctx_h, ctok),
        (ngain_h, ngain),
        (wup_h, wup),
        (kgain_h, kgain),
        (qgain_h, qgain),
        (kvgain_h, kvgain),
        (wdown_h, wdown),
        (wrope_h, wrope),
        (wq_h, wq),
        (wout_h, wout),
    ]
    loads = [pltpu.make_async_copy(a, b, load_sem.at[i]) for i, (a, b) in enumerate(pairs)]
    for copy in loads:
        copy.start()

    barrier = pltpu.get_barrier_semaphore()
    peers = (
        [z_peer(k) for k in range(1, nz)]
        + [y_peer(k) for k in range(1, ny)]
        + [t_peer(k) for k in range(1, ntp)]
    )
    for peer in peers:
        pl.semaphore_signal(barrier, inc=1, device_id=peer, device_id_type=MESH)

    for i in range(5):
        loads[i].wait()
    mod_rows = mods.shape[1]
    fold = LANES // mod_rows
    quarter = sp % fold
    own_row = sp // fold
    lat_row = silu(cond_v[pl.ds(own_row, 1), :])
    ctx_row = silu(cctx_v[pl.ds(own_row, 1), :])
    mine = lane_ids((1, LANES)) // mod_rows == quarter
    signal = jnp.concatenate(
        [jnp.where(mine, lat_row, 0.0), jnp.where(mine, ctx_row, 0.0), jnp.zeros((6, LANES), F32)],
        axis=0,
    )
    block = jnp.concatenate([mods[0], mods[1], mods[2]], axis=1).astype(F32)
    block = jnp.concatenate([block] * fold, axis=0)
    share = jnp.dot(signal, block, precision=HIGHEST, preferred_element_type=F32)
    zbuf[0] = share[0:2, : 2 * piece]
    gzbuf[0] = share[0:1, 2 * piece :]

    pl.semaphore_wait(barrier, len(peers))

    sent = []

    def remote(src, dst, index, device):
        return Flight(
            sent,
            pltpu.make_async_remote_copy(
                src_ref=src,
                dst_ref=dst,
                send_sem=send_sem.at[index],
                recv_sem=recv_sem.at[index],
                device_id=device,
                device_id_type=MESH,
            ),
        )

    def far_first(count):
        return sorted(range(1, count), key=lambda k: -min(k, count - k))

    def exchange(buf, count, peer, first):
        return [remote(buf.at[0], buf.at[k], first + k, peer(k)) for k in far_first(count)]

    def spread_tp(buf, first):
        return [remote(buf.at[tp], buf.at[tp], first + k, t_peer(k)) for k in range(1, ntp)]

    def direct(count):
        if count < 8:
            return list(range(1, count))
        return [2, count - 2, 1, count - 1]

    def landed(flights):
        for flight in flights:
            flight.wait_recv()

    z_copies = exchange(zbuf, nz, z_peer, 0)
    gz_copies = exchange(gzbuf, nz, z_peer, 8)

    loads[5].wait()
    near_x = sorted({k for k in (1, ntp // 2 - 1) if 0 < k < ntp // 2})
    tok_near = {k: remote(gtok.at[tp], gtok.at[tp], 16 + k, x_peer(k)) for k in near_x}
    tok_side = [remote(gtok.at[tp], gtok.at[tp], 16, sibling)]
    tok_half = []

    for i in range(6, 12):
        loads[i].wait()
    gain_row = ngain[...]
    cv = ctok[...].astype(F32)
    nvc[...] = cv * lax.rsqrt(jnp.mean(cv * cv, axis=1, keepdims=True) + EPS) * gain_row
    wupt[...] = wup[0].astype(F32).T.astype(BF16)
    keys[...] = jnp.zeros(keys.shape, BF16)
    vals[:, nlat:, :] = jnp.zeros((2, LANES, LANES), BF16)
    ctxl[...] = jnp.zeros(ctxl.shape, F32)
    ctxr[...] = jnp.zeros(ctxr.shape, F32)
    msg[0, :, 64:80, :] = jnp.zeros((2, 16, KVL), BF16)
    hid[LANES:, :] = jnp.zeros((hid.shape[0] - LANES, width), BF16)
    kg = column_tile(kgain[...])
    qg = column_tile(qgain[...]) * (LOG2E * QK ** (-0.5))
    for k in range(nz):
        cosine, sine = angle_tables(((zi + nz - k) % nz) * ny + yi)
        ctab[k] = cosine
        stab[k] = sine

    for k in near_x:
        tok_near[k].wait_recv()
        came = x_index(ntp // 2 - k)
        if ntp // 2 == 4:
            lanes = pl.ds(0 if k == 1 else width // 2, width // 2)
            tok_half.append(
                remote(gtok.at[came, :, lanes], gtok.at[came, :, lanes], 20 + k, x_peer(k))
            )
        tok_side.append(remote(gtok.at[came], gtok.at[came], 24 + k, sibling))

    landed(z_copies)
    total = zbuf[0]
    for k in range(1, nz):
        total = total + zbuf[k]
    ybuf[0] = total
    y_copies = exchange(ybuf, ny, y_peer, 32)
    landed(gz_copies)
    total = gzbuf[0]
    for k in range(1, nz):
        total = total + gzbuf[k]
    gybuf[0] = total
    gy_copies = exchange(gybuf, ny, y_peer, 40)

    if tok_half:
        landed(tok_half)
        far = x_index(2)
        tok_side.append(remote(gtok.at[far], gtok.at[far], 28, sibling))
    landed(y_copies)
    total = ybuf[0]
    for k in range(1, ny):
        total = total + ybuf[k]
    tbuf[tp] = total

    t_copies = spread_tp(tbuf, 48)
    landed(gy_copies)
    total = gybuf[0]
    for k in range(1, ny):
        total = total + gybuf[k]
    gtbuf[tp] = total
    gt_copies = spread_tp(gtbuf, 56)

    landed(tok_side)

    def norm_rows(i, carry):
        v = gtok[i].astype(F32)
        scaled = v * lax.rsqrt(jnp.mean(v * v, axis=1, keepdims=True) + EPS) * gain_row
        nv[pl.ds(pl.multiple_of(i * rows, rows), rows), :] = scaled
        return carry

    lax.fori_loop(0, ntp, norm_rows, 0)

    for i in range(12, 16):
        loads[i].wait()
    landed(t_copies)

    def vector(which, who):
        return jnp.concatenate(
            [tbuf[t][who : who + 1, which * piece : (which + 1) * piece] for t in range(ntp)],
            axis=1,
        )

    shift_row = vector(0, 0)
    scale_row = 1.0 + vector(1, 0)

    def modulate(i, carry):
        at = pl.ds(pl.multiple_of(i * 16, 16), 16)
        hid[at, :] = (nv[at, :] * scale_row + shift_row).astype(BF16)
        return carry

    lax.fori_loop(0, LANES // 16, modulate, 0)
    ctx_hidden = nvc[...] * (1.0 + vector(1, 1)) + vector(0, 1)
    hid[LANES : LANES + 16, :] = jnp.concatenate(
        [ctx_hidden, jnp.zeros((16 - crow, width), F32)], axis=0
    ).astype(BF16)

    raw = jnp.dot(hid[...], wdown[...], preferred_element_type=F32)
    lat = raw * lax.rsqrt(jnp.mean(raw * raw, axis=1, keepdims=True) + EPS) * kvgain[...]
    rope_t = nt_dot(wrope[...], hid[:LANES, :])
    rope_c = nt_dot(hid[LANES:, :], wrope[...])
    rope_c = jnp.concatenate([rope_c, jnp.zeros((16, LANES - ROPE), F32)], axis=1)
    ctx_lat = lat[LANES : LANES + crow]
    msg[0, 0, 0:64, :] = lat[0:64].astype(BF16)
    msg[0, 1, 0:64, :] = lat[64:128].astype(BF16)
    msg[0, 0, 64:80, 0:LANES] = rope_t[:16].astype(BF16)
    msg[0, 1, 64:80, 0:LANES] = rope_t[16:].astype(BF16)
    msg[0, 0, 64:80, LANES:] = jnp.concatenate([ctx_lat[:, :LANES], ctx_lat[:, LANES:]], axis=0).astype(BF16)
    msg[0, 1, 64:80, LANES:] = rope_c.astype(BF16)
    k_near = {
        k: remote(msg.at[0, core], msg.at[k, core], 64 + k, z_peer(k)) for k in direct(nz)
    }

    raw_t = nt_dot(wq[...], hid[:LANES, :])
    plains, tails = [], []
    for h in range(2):
        u = raw_t[h * QK : (h + 1) * QK]
        inv = lax.rsqrt(jnp.sum(u * u, axis=0, keepdims=True) * (1.0 / QK) + EPS)
        u = u * inv * qg[:QK]
        plains.append(u[:HD])
        tails.append(rotated(u[HD:], ctab[0], stab[0]))
    plain = jnp.concatenate(plains, axis=0).T
    tail = jnp.concatenate(tails, axis=0)
    tail = jnp.concatenate([tail, pltpu.roll(tail, LANES // 2, 1)], axis=0).T
    qbuf[0, 0:LANES, :] = plain.astype(BF16)
    qbuf[0, LANES:, :] = tail[: LANES // 2].astype(BF16)
    q_near = {k: remote(qbuf.at[0], qbuf.at[k], 80 + k, y_peer(k)) for k in direct(ny)}

    def expand_slot(k):
        latent = msg[k, :, 0:64, :].reshape(LANES, KVL)
        rope_k = jnp.concatenate([msg[k, 0, 64:80, 0:LANES], msg[k, 1, 64:80, 0:LANES]], axis=0).astype(F32)
        up = nt_dot(wupt[...], latent)
        shared = jnp.sum(rope_k * rope_k, axis=0, keepdims=True)
        at = pl.ds(k * LANES, LANES)
        for h in range(2):
            part = up[h * HD : (h + 1) * HD]
            inv = lax.rsqrt((jnp.sum(part * part, axis=0, keepdims=True) + shared) * (1.0 / QK) + EPS)
            keys[h, h * HD : (h + 1) * HD, at] = (part * inv * kg[:HD]).astype(BF16)
            turned = rotated(rope_k * inv * kg[HD:QK], ctab[k], stab[k])
            keys[h, LANES + h * ROPE : LANES + (h + 1) * ROPE, at] = turned.astype(BF16)
        value = jnp.dot(latent, wup[1], preferred_element_type=F32)
        low = lane_ids((LANES, LANES)) < HD
        vals[0, at, :] = jnp.where(low, value, 1.0).astype(BF16)
        vals[1, at, :] = jnp.where(low, 1.0, value).astype(BF16)
        ctx_two = msg[k, 0, 64:80, LANES:].astype(F32)
        ctxl[k * crow : (k + 1) * crow, :] = jnp.concatenate([ctx_two[:crow], ctx_two[8 : 8 + crow]], axis=1)
        ctxr[k * crow : (k + 1) * crow, :] = msg[k, 1, 64:80, LANES:].astype(F32)[:crow]

    expand_slot(0)
    def relay(near, buf, whole, part, count, peer, first):
        if count < 8:
            return {}
        for k in (2, count - 2):
            near[k].wait_recv()
        out = {count // 2: []}
        for side, k, step in ((0, 2, 1), (1, count - 2, count - 1)):
            onward = (k + step) % count
            out[onward] = [remote(whole(buf.at[k]), whole(buf.at[onward]), first + onward, peer(step))]
        for side, k in ((0, 2), (1, count - 2)):
            out[count // 2].append(
                remote(part(buf.at[k], side), part(buf.at[count // 2], side), first + 8 + side, peer(k))
            )
        return out

    def key_whole(ref):
        return ref.at[core]

    def key_part(ref, side):
        return ref.at[core, :, pl.ds(side * LANES, LANES)]

    def query_whole(ref):
        return ref

    def query_part(ref, side):
        return ref.at[pl.ds(side * (qrows // 2), qrows // 2), :]

    qrows = qbuf.shape[1]
    k_far = relay(k_near, msg, key_whole, key_part, nz, z_peer, 96)
    q_far = relay(q_near, qbuf, query_whole, query_part, ny, y_peer, 112)
    arrivals = {k: [k_near[k]] for k in direct(nz)}
    arrivals.update(k_far)
    forwards = []
    order = direct(nz) + sorted(k_far, key=lambda k: min(k, nz - k))
    for k in order:
        landed(f for f in arrivals[k] if not f.landed)
        forwards.append(remote(msg.at[k, core], msg.at[k, core], 128 + k, sibling))
        if len(forwards) > 1:
            forwards[-2].wait_recv()
            expand_slot(order[len(forwards) - 2])
    if forwards:
        forwards[-1].wait_recv()
        expand_slot(order[-1])

    latent = ctxl[...].astype(BF16)
    rope_k = ctxr[...].T[:ROPE]
    up = nt_dot(wupt[...], latent)
    shared = jnp.sum(rope_k * rope_k, axis=0, keepdims=True)
    at = pl.ds(nlat, LANES)
    for h in range(2):
        part = up[h * HD : (h + 1) * HD]
        inv = lax.rsqrt((jnp.sum(part * part, axis=0, keepdims=True) + shared) * (1.0 / QK) + EPS)
        keys[h, h * HD : (h + 1) * HD, at] = (part * inv * kg[:HD]).astype(BF16)
        keys[h, LANES + h * ROPE : LANES + (h + 1) * ROPE, at] = (rope_k * inv * kg[HD:QK]).astype(BF16)
    value = jnp.dot(latent, wup[1], preferred_element_type=F32)
    low = lane_ids((LANES, LANES)) < HD
    real = row_ids((LANES, LANES)) < nz * crow
    ones = jnp.where(real, 1.0, 0.0)
    vals[0, at, :] = jnp.where(low, value, ones).astype(BF16)
    vals[1, at, :] = jnp.where(low, ones, value).astype(BF16)

    diagonal = lane_ids((LANES, LANES)) % HD == row_ids((LANES, LANES)) % HD

    low = lane_ids((LANES, LANES)) < HD
    late = lane_ids((1, nlat + LANES)) < nlat
    lifts = [jnp.where(late, lift_s[0, h] * LOG2E, 0.0) for h in range(2)]

    def whole_query(j):
        tails = qbuf[j, LANES:, :]
        turned_tails = pltpu.roll(tails.astype(F32), LANES // 2, 1).astype(BF16)
        return jnp.concatenate([qbuf[j, 0:LANES, :], jnp.concatenate([tails, turned_tails], axis=0)], axis=1)

    def attend(slots):
        q = jnp.concatenate([whole_query(j) for j in slots], axis=0)
        outs = []
        for h in range(2):
            p = jnp.exp2(jnp.dot(q, keys[h], preferred_element_type=F32) - lifts[h]).astype(BF16)
            outs.append(jnp.dot(p, vals[h], preferred_element_type=F32))
        for i, j in enumerate(slots):
            first, second = (out[i * LANES : (i + 1) * LANES] for out in outs)
            den = jnp.where(diagonal, jnp.where(low, second, first), 0.0)
            packed = jnp.concatenate(
                [
                    jnp.sum(den[:HD], axis=0, keepdims=True),
                    jnp.sum(den[HD:], axis=0, keepdims=True),
                ],
                axis=0,
            )
            hi = packed.astype(BF16).astype(F32)
            lo = packed - hi
            ostage[j, 0:LANES, :] = jnp.where(low, first, second).astype(BF16)
            ostage[j, LANES:, :] = jnp.concatenate([hi, lo, jnp.zeros((12, LANES), F32)], axis=0).astype(BF16)

    o_copies = []
    o_half = []
    halves = ((0, HD), (HD, ostage.shape[1] - HD))
    order = sorted(range(ny), key=lambda j: -min(j, ny - j))
    arrivals = {k: [q_near[k]] for k in direct(ny)}
    arrivals.update(q_far)
    arrivals[0] = []
    for at in range(0, ny, 2):
        slots = order[at : at + 2]
        for j in slots:
            landed(f for f in arrivals[j] if not f.landed)
        attend(slots)
        for j in slots:
            if j == 4:
                for side, step in ((0, 2), (1, ny - 2)):
                    rows_at = pl.ds(*halves[side])
                    o_half.append(
                        remote(ostage.at[j, rows_at, :], opass.at[rows_at, :], 138 + side, y_peer(step))
                    )
            elif j:
                o_copies.append(remote(ostage.at[j], obuf.at[j], 144 + j, y_peer(ny - j)))
    if o_half:
        for side, step in ((0, 2), (1, ny - 2)):
            o_half[side].wait_recv()
            rows_at = pl.ds(*halves[side])
            o_copies.append(remote(opass.at[rows_at, :], obuf.at[4, rows_at, :], 152 + side, y_peer(step)))
    landed(o_copies)
    num = ostage[0, 0:LANES, :].astype(F32)
    den = ostage[0, LANES:, :].astype(F32)
    for j in range(1, ny):
        num = num + obuf[j, 0:LANES, :].astype(F32)
        den = den + obuf[j, LANES:, :].astype(F32)
    den = den[0:2] + den[2:4]
    spread = jnp.concatenate(
        [
            jnp.broadcast_to(den[0:1], (HD, LANES)),
            jnp.broadcast_to(den[1:2], (HD, LANES)),
        ],
        axis=0,
    )
    spread = jnp.where(diagonal, spread, 0.0)
    swap = jnp.where((lane_ids((LANES, LANES)) < HD) != (row_ids((LANES, LANES)) < HD), 1.0, 0.0)
    spread = jnp.dot(spread, swap, precision=HIGHEST, preferred_element_type=F32)
    attended = (num / spread).astype(BF16)

    proj = jnp.dot(attended, wout[...], preferred_element_type=F32).astype(BF16)
    for t in range(ntp):
        rstage[t] = proj[t * rows : (t + 1) * rows]
    r_copies = [
        remote(rstage.at[(tp + k) % ntp], rbuf.at[k], 160 + k, t_peer(k)) for k in range(1, ntp)
    ]
    result = rstage[tp].astype(F32)
    landed(r_copies)
    for k in range(1, ntp):
        result = result + rbuf[k].astype(F32)
    landed(gt_copies)
    gate_row = jnp.concatenate([gtbuf[t] for t in range(ntp)], axis=1)
    out_ref[...] = (gtok[tp].astype(F32) + gate_row * result).astype(BF16)

    for flight in sent:
        flight.wait_send()


def solution(mesh, nz=8):
    nsp, ntp = mesh.shape["sp"], mesh.shape["tp"]
    ny = nsp // nz

    def local(
        latent_tokens,
        context_tokens,
        cond,
        ctx_cond,
        mod_shift,
        mod_scale,
        mod_gate,
        norm_gain,
        w_query,
        query_gain,
        w_down_kv,
        w_rope_key,
        kv_gain,
        w_up_kv,
        key_gain,
        ctx_lift,
        w_output,
    ):
        rows, width = latent_tokens.shape
        crow = context_tokens.shape[0]
        piece = mod_shift.shape[1]
        lat = nz * LANES
        vm = pltpu.VMEM
        anywhere = pl.BlockSpec(memory_space=pl.ANY)
        smem = pl.BlockSpec(memory_space=pltpu.SMEM)
        return pl.pallas_call(
            functools.partial(kernel, nz, ny, ntp),
            out_shape=jax.ShapeDtypeStruct((rows, width), BF16),
            in_specs=[anywhere] * 15 + [smem, anywhere],
            out_specs=pl.BlockSpec(memory_space=pltpu.VMEM),
            scratch_shapes=[
                vm((ntp, rows, width), BF16),
                vm((crow, width), BF16),
                vm((width // LANES, LANES), F32),
                vm((width // LANES, LANES), F32),
                vm((3, mod_shift.shape[0], piece), BF16),
                vm((1, width), F32),
                vm(w_query.shape[::-1], BF16),
                vm((1, QK), F32),
                vm(w_down_kv.shape, BF16),
                vm(w_rope_key.shape[::-1], BF16),
                vm((1, KVL), F32),
                vm(w_up_kv.shape, BF16),
                vm((1, QK), F32),
                vm(w_output.shape, BF16),
                vm((nz, 2, 2 * piece), F32),
                vm((ny, 2, 2 * piece), F32),
                vm((ntp, 2, 2 * piece), F32),
                vm((nz, 1, piece), F32),
                vm((ny, 1, piece), F32),
                vm((ntp, 1, piece), F32),
                vm((LANES, width), F32),
                vm((crow, width), F32),
                vm((LANES + 16, width), BF16),
                vm((LANES, KVL), BF16),
                vm((nz, HALF, LANES), F32),
                vm((nz, HALF, LANES), F32),
                vm((nz, 2, MSG, KVL), BF16),
                vm((ny, LANES + HD, LANES), BF16),
                vm((2, 2 * LANES, lat + LANES), BF16),
                vm((2, lat + LANES, LANES), BF16),
                vm((LANES, KVL), F32),
                vm((LANES, LANES), F32),
                vm((ny, LANES + 16, LANES), BF16),
                vm((ny, LANES + 16, LANES), BF16),
                vm((LANES + 16, LANES), BF16),
                vm((ntp, rows, width), BF16),
                vm((ntp, rows, width), BF16),
                pltpu.SemaphoreType.DMA((16,)),
                pltpu.SemaphoreType.DMA((176,)),
                pltpu.SemaphoreType.DMA((176,)),
            ],
            compiler_params=pltpu.CompilerParams(
                collective_id=0, has_side_effects=True, vmem_limit_bytes=60 * 1024 * 1024
            ),
        )(
            latent_tokens,
            context_tokens,
            cond.reshape(width // LANES, LANES),
            ctx_cond.reshape(width // LANES, LANES),
            mod_shift,
            mod_scale,
            mod_gate,
            norm_gain.reshape(1, width),
            w_query.T,
            query_gain.reshape(1, QK),
            w_down_kv,
            w_rope_key.T,
            kv_gain.reshape(1, KVL),
            w_up_kv,
            key_gain.reshape(1, QK),
            ctx_lift.reshape(1, 2),
            w_output,
        )

    in_specs = (
        P(("sp", "tp"), None),
        P("sp", None),
        P(),
        P(),
        P("sp", "tp"),
        P("sp", "tp"),
        P("sp", "tp"),
        P(),
        P(None, "tp"),
        P(),
        P(),
        P(),
        P(),
        P(None, None, "tp"),
        P(),
        P("tp"),
        P("tp", None),
    )
    return jax.shard_map(local, mesh=mesh, in_specs=in_specs, out_specs=P(("sp", "tp"), None), check_vma=False)
```

```python
import functools
import math

import jax
import jax.numpy as jnp
from jax import lax
from jax.experimental import pallas as pl
from jax.experimental.pallas import tpu as pltpu
from jax.sharding import PartitionSpec as P

HD = 64
ROPE = 32
QK = 96
KVL = 256
HALF = ROPE // 2
GRID_W = 64
EPS = 1e-06
THETA = 10000.0
LOG2E = math.log2(math.e)
MESH = pl.DeviceIdType.MESH
F32 = jnp.float32
BF16 = jnp.bfloat16
HIGHEST = lax.Precision.HIGHEST
LANES = 128
MSG = 80


def nt_dot(a, b):
    return lax.dot_general(a, b, (((1,), (1,)), ((), ())), preferred_element_type=F32)


def lane_ids(shape):
    return lax.broadcasted_iota(jnp.int32, shape, 1)


def row_ids(shape):
    return lax.broadcasted_iota(jnp.int32, shape, 0)


def silu(v):
    return v / (1.0 + jnp.exp(-v))


def column_tile(row):
    width = row.shape[1]
    full = jnp.concatenate([row, jnp.zeros((1, LANES - width), F32)], axis=1)
    return jnp.broadcast_to(full, (LANES, LANES)).T


class Flight:
    def __init__(self, sent, copy):
        self.copy, self.landed = copy, False
        sent.append(self)
        copy.start()

    def wait_recv(self):
        self.landed = True
        self.copy.wait_recv()

    def wait_send(self):
        self.copy.wait_send()


def angle_tables(group):
    shape = (HALF, LANES)
    freq_row = row_ids(shape)
    token = lane_ids(shape)
    inverse = jnp.zeros(shape, F32)
    for j in range(HALF // 2):
        inverse = jnp.where(freq_row % (HALF // 2) == j, THETA ** (-j / (HALF // 2)), inverse)
    row = (group * (LANES // GRID_W) + token // GRID_W).astype(F32)
    col = (token % GRID_W).astype(F32)
    angle = jnp.where(freq_row < HALF // 2, row, col) * inverse
    return jnp.cos(angle), jnp.sin(angle)


def rotated(tail, cosine, sine):
    front, back = tail[:HALF], tail[HALF:]
    return jnp.concatenate([front * cosine - back * sine, back * cosine + front * sine], axis=0)


def kernel(
    nz,
    ny,
    ntp,
    tok_h,
    ctx_h,
    cond_h,
    cctx_h,
    mshift_h,
    mscale_h,
    mgate_h,
    ngain_h,
    wq_h,
    qgain_h,
    wdown_h,
    wrope_h,
    kvgain_h,
    wup_h,
    kgain_h,
    lift_s,
    wout_h,
    out_ref,
    gtok,
    ctok,
    cond_v,
    cctx_v,
    mods,
    ngain,
    wq,
    qgain,
    wdown,
    wrope,
    kvgain,
    wup,
    kgain,
    wout,
    zbuf,
    ybuf,
    tbuf,
    gzbuf,
    gybuf,
    gtbuf,
    nv,
    nvc,
    hid,
    wupt,
    ctab,
    stab,
    msg,
    qbuf,
    keys,
    vals,
    ctxl,
    ctxr,
    ostage,
    obuf,
    opass,
    share_out,
    heads,
    load_sem,
    send_sem,
    recv_sem,
):
    sp = lax.axis_index("sp")
    tp = lax.axis_index("tp")
    zi, yi = sp // ny, sp % ny
    core = tp % 2
    rows = tok_h.shape[0]
    width = tok_h.shape[1]
    piece = mods.shape[2]
    crow = ctx_h.shape[0]
    nlat = nz * LANES

    def z_peer(k):
        return (((zi + k) % nz) * ny + yi, tp)

    def y_peer(k):
        return (zi * ny + (yi + k) % ny, tp)

    def t_peer(k):
        return (sp, (tp + k) % ntp)

    sibling = (sp, tp + 1 - 2 * core)

    def x_index(k):
        return (tp + 2 * k) % ntp

    def x_peer(k):
        return (sp, x_index(k))

    pairs = [
        (cond_h, cond_v),
        (cctx_h, cctx_v),
        (mshift_h, mods.at[0]),
        (mscale_h, mods.at[1]),
        (mgate_h, mods.at[2]),
        (tok_h, gtok.at[tp]),
        (ctx_h, ctok),
        (ngain_h, ngain),
        (wup_h, wup),
        (kgain_h, kgain),
        (qgain_h, qgain),
        (kvgain_h, kvgain),
        (wdown_h, wdown),
        (wrope_h, wrope),
        (wq_h, wq),
        (wout_h, wout.at[tp]),
    ]
    loads = [pltpu.make_async_copy(a, b, load_sem.at[i]) for i, (a, b) in enumerate(pairs)]
    for copy in loads:
        copy.start()

    barrier = pltpu.get_barrier_semaphore()
    peers = (
        [z_peer(k) for k in range(1, nz)]
        + [y_peer(k) for k in range(1, ny)]
        + [t_peer(k) for k in range(1, ntp)]
    )
    for peer in peers:
        pl.semaphore_signal(barrier, inc=1, device_id=peer, device_id_type=MESH)

    for i in range(5):
        loads[i].wait()
    mod_rows = mods.shape[1]
    fold = LANES // mod_rows
    quarter = sp % fold
    own_row = sp // fold
    lat_row = silu(cond_v[pl.ds(own_row, 1), :])
    ctx_row = silu(cctx_v[pl.ds(own_row, 1), :])
    mine = lane_ids((1, LANES)) // mod_rows == quarter
    signal = jnp.concatenate(
        [jnp.where(mine, lat_row, 0.0), jnp.where(mine, ctx_row, 0.0), jnp.zeros((6, LANES), F32)],
        axis=0,
    )
    block = jnp.concatenate([mods[0], mods[1], mods[2]], axis=1).astype(F32)
    block = jnp.concatenate([block] * fold, axis=0)
    share = jnp.dot(signal, block, precision=HIGHEST, preferred_element_type=F32)
    zbuf[0] = share[0:2, : 2 * piece]
    gzbuf[0] = share[0:1, 2 * piece :]

    pl.semaphore_wait(barrier, len(peers))

    sent = []

    def remote(src, dst, index, device):
        return Flight(
            sent,
            pltpu.make_async_remote_copy(
                src_ref=src,
                dst_ref=dst,
                send_sem=send_sem.at[index],
                recv_sem=recv_sem.at[index],
                device_id=device,
                device_id_type=MESH,
            ),
        )

    def far_first(count):
        return sorted(range(1, count), key=lambda k: -min(k, count - k))

    def exchange(buf, count, peer, first):
        return [remote(buf.at[0], buf.at[k], first + k, peer(k)) for k in far_first(count)]

    def spread_tp(buf, first):
        return [remote(buf.at[tp], buf.at[tp], first + k, t_peer(k)) for k in range(1, ntp)]

    def direct(count):
        if count < 8:
            return list(range(1, count))
        return [2, count - 2, 1, count - 1]

    def landed(flights):
        for flight in flights:
            flight.wait_recv()

    z_copies = exchange(zbuf, nz, z_peer, 0)
    gz_copies = exchange(gzbuf, nz, z_peer, 8)

    loads[5].wait()
    near_x = sorted({k for k in (1, ntp // 2 - 1) if 0 < k < ntp // 2})
    tok_near = {k: remote(gtok.at[tp], gtok.at[tp], 16 + k, x_peer(k)) for k in near_x}
    tok_side = [remote(gtok.at[tp], gtok.at[tp], 16, sibling)]
    tok_half = []

    for i in range(6, 12):
        loads[i].wait()
    gain_row = ngain[...]
    cv = ctok[...].astype(F32)
    nvc[...] = cv * lax.rsqrt(jnp.mean(cv * cv, axis=1, keepdims=True) + EPS) * gain_row
    wupt[...] = wup[0].astype(F32).T.astype(BF16)
    keys[...] = jnp.zeros(keys.shape, BF16)
    vals[:, nlat:, :] = jnp.zeros((2, LANES, LANES), BF16)
    ctxl[...] = jnp.zeros(ctxl.shape, F32)
    ctxr[...] = jnp.zeros(ctxr.shape, F32)
    msg[0, :, 64:80, :] = jnp.zeros((2, 16, KVL), BF16)
    hid[LANES:, :] = jnp.zeros((hid.shape[0] - LANES, width), BF16)
    kg = column_tile(kgain[...])
    qg = column_tile(qgain[...]) * (LOG2E * QK ** (-0.5))
    for k in range(nz):
        cosine, sine = angle_tables(((zi + nz - k) % nz) * ny + yi)
        ctab[k] = cosine
        stab[k] = sine

    for k in near_x:
        tok_near[k].wait_recv()
        came = x_index(ntp // 2 - k)
        if ntp // 2 == 4:
            lanes = pl.ds(0 if k == 1 else width // 2, width // 2)
            tok_half.append(
                remote(gtok.at[came, :, lanes], gtok.at[came, :, lanes], 20 + k, x_peer(k))
            )
        tok_side.append(remote(gtok.at[came], gtok.at[came], 24 + k, sibling))

    nx = ntp // 2
    half_w = width // 2

    def columns(side):
        return pl.ds(side * half_w, half_w)

    def w_block(index, side):
        return wout.at[index, :, columns(side)]

    loads[15].wait()
    w_side = [remote(wout.at[tp], wout.at[tp], 168, sibling)]
    w_first = {k: remote(w_block(tp, side), w_block(tp, side), 169 + side, x_peer(k)) for side, k in enumerate(near_x)}

    landed(z_copies)
    total = zbuf[0]
    for k in range(1, nz):
        total = total + zbuf[k]
    ybuf[0] = total
    y_copies = exchange(ybuf, ny, y_peer, 32)
    landed(gz_copies)
    total = gzbuf[0]
    for k in range(1, nz):
        total = total + gzbuf[k]
    gybuf[0] = total
    gy_copies = exchange(gybuf, ny, y_peer, 40)

    if tok_half:
        landed(tok_half)
        far = x_index(2)
        tok_side.append(remote(gtok.at[far], gtok.at[far], 28, sibling))
    landed(y_copies)
    total = ybuf[0]
    for k in range(1, ny):
        total = total + ybuf[k]
    tbuf[tp] = total

    t_copies = spread_tp(tbuf, 48)
    landed(gy_copies)
    total = gybuf[0]
    for k in range(1, ny):
        total = total + gybuf[k]
    gtbuf[tp] = total
    gt_copies = spread_tp(gtbuf, 56)

    landed(tok_side)

    def norm_rows(i, carry):
        v = gtok[i].astype(F32)
        scaled = v * lax.rsqrt(jnp.mean(v * v, axis=1, keepdims=True) + EPS) * gain_row
        nv[pl.ds(pl.multiple_of(i * rows, rows), rows), :] = scaled
        return carry

    lax.fori_loop(0, ntp, norm_rows, 0)

    for i in range(12, 15):
        loads[i].wait()
    landed(t_copies)
    w_second = {k: remote(w_block(tp, 1 - side), w_block(tp, 1 - side), 171 + side, x_peer(k)) for side, k in enumerate(near_x)}
    w_far = []
    if nx == 4:
        for side, k in enumerate(near_x):
            w_first[k].wait_recv()
            came = x_index(nx - k)
            w_far.append(remote(w_block(came, side), w_block(came, side), 173 + side, x_peer(k)))

    def vector(which, who):
        return jnp.concatenate(
            [tbuf[t][who : who + 1, which * piece : (which + 1) * piece] for t in range(ntp)],
            axis=1,
        )

    shift_row = vector(0, 0)
    scale_row = 1.0 + vector(1, 0)

    def modulate(i, carry):
        at = pl.ds(pl.multiple_of(i * 16, 16), 16)
        hid[at, :] = (nv[at, :] * scale_row + shift_row).astype(BF16)
        return carry

    lax.fori_loop(0, LANES // 16, modulate, 0)
    ctx_hidden = nvc[...] * (1.0 + vector(1, 1)) + vector(0, 1)
    hid[LANES : LANES + 16, :] = jnp.concatenate(
        [ctx_hidden, jnp.zeros((16 - crow, width), F32)], axis=0
    ).astype(BF16)

    raw = jnp.dot(hid[...], wdown[...], preferred_element_type=F32)
    lat = raw * lax.rsqrt(jnp.mean(raw * raw, axis=1, keepdims=True) + EPS) * kvgain[...]
    rope_t = nt_dot(wrope[...], hid[:LANES, :])
    rope_c = nt_dot(hid[LANES:, :], wrope[...])
    rope_c = jnp.concatenate([rope_c, jnp.zeros((16, LANES - ROPE), F32)], axis=1)
    ctx_lat = lat[LANES : LANES + crow]
    msg[0, 0, 0:64, :] = lat[0:64].astype(BF16)
    msg[0, 1, 0:64, :] = lat[64:128].astype(BF16)
    msg[0, 0, 64:80, 0:LANES] = rope_t[:16].astype(BF16)
    msg[0, 1, 64:80, 0:LANES] = rope_t[16:].astype(BF16)
    msg[0, 0, 64:80, LANES:] = jnp.concatenate([ctx_lat[:, :LANES], ctx_lat[:, LANES:]], axis=0).astype(BF16)
    msg[0, 1, 64:80, LANES:] = rope_c.astype(BF16)
    k_near = {
        k: remote(msg.at[0, core], msg.at[k, core], 64 + k, z_peer(k)) for k in direct(nz)
    }

    raw_t = nt_dot(wq[...], hid[:LANES, :])
    plains, tails = [], []
    for h in range(2):
        u = raw_t[h * QK : (h + 1) * QK]
        inv = lax.rsqrt(jnp.sum(u * u, axis=0, keepdims=True) * (1.0 / QK) + EPS)
        u = u * inv * qg[:QK]
        plains.append(u[:HD])
        tails.append(rotated(u[HD:], ctab[0], stab[0]))
    plain = jnp.concatenate(plains, axis=0).T
    tail = jnp.concatenate(tails, axis=0)
    tail = jnp.concatenate([tail, pltpu.roll(tail, LANES // 2, 1)], axis=0).T
    qbuf[0, 0:LANES, :] = plain.astype(BF16)
    qbuf[0, LANES:, :] = tail[: LANES // 2].astype(BF16)
    q_near = {k: remote(qbuf.at[0], qbuf.at[k], 80 + k, y_peer(k)) for k in direct(ny)}

    def expand_slot(k):
        latent = msg[k, :, 0:64, :].reshape(LANES, KVL)
        rope_k = jnp.concatenate([msg[k, 0, 64:80, 0:LANES], msg[k, 1, 64:80, 0:LANES]], axis=0).astype(F32)
        up = nt_dot(wupt[...], latent)
        shared = jnp.sum(rope_k * rope_k, axis=0, keepdims=True)
        at = pl.ds(k * LANES, LANES)
        for h in range(2):
            part = up[h * HD : (h + 1) * HD]
            inv = lax.rsqrt((jnp.sum(part * part, axis=0, keepdims=True) + shared) * (1.0 / QK) + EPS)
            keys[h, h * HD : (h + 1) * HD, at] = (part * inv * kg[:HD]).astype(BF16)
            turned = rotated(rope_k * inv * kg[HD:QK], ctab[k], stab[k])
            keys[h, LANES + h * ROPE : LANES + (h + 1) * ROPE, at] = turned.astype(BF16)
        value = jnp.dot(latent, wup[1], preferred_element_type=F32)
        low = lane_ids((LANES, LANES)) < HD
        vals[0, at, :] = jnp.where(low, value, 1.0).astype(BF16)
        vals[1, at, :] = jnp.where(low, 1.0, value).astype(BF16)
        ctx_two = msg[k, 0, 64:80, LANES:].astype(F32)
        ctxl[k * crow : (k + 1) * crow, :] = jnp.concatenate([ctx_two[:crow], ctx_two[8 : 8 + crow]], axis=1)
        ctxr[k * crow : (k + 1) * crow, :] = msg[k, 1, 64:80, LANES:].astype(F32)[:crow]

    expand_slot(0)
    def relay(near, buf, whole, part, count, peer, first):
        if count < 8:
            return {}
        for k in (2, count - 2):
            near[k].wait_recv()
        out = {count // 2: []}
        for side, k, step in ((0, 2, 1), (1, count - 2, count - 1)):
            onward = (k + step) % count
            out[onward] = [remote(whole(buf.at[k]), whole(buf.at[onward]), first + onward, peer(step))]
        for side, k in ((0, 2), (1, count - 2)):
            out[count // 2].append(
                remote(part(buf.at[k], side), part(buf.at[count // 2], side), first + 8 + side, peer(k))
            )
        return out

    def key_whole(ref):
        return ref.at[core]

    def key_part(ref, side):
        return ref.at[core, :, pl.ds(side * LANES, LANES)]

    def query_whole(ref):
        return ref

    def query_part(ref, side):
        return ref.at[pl.ds(side * (qrows // 2), qrows // 2), :]

    qrows = qbuf.shape[1]
    k_far = relay(k_near, msg, key_whole, key_part, nz, z_peer, 96)
    q_far = relay(q_near, qbuf, query_whole, query_part, ny, y_peer, 112)
    arrivals = {k: [k_near[k]] for k in direct(nz)}
    arrivals.update(k_far)
    forwards = []
    order = direct(nz) + sorted(k_far, key=lambda k: min(k, nz - k))
    for k in order:
        landed(f for f in arrivals[k] if not f.landed)
        forwards.append(remote(msg.at[k, core], msg.at[k, core], 128 + k, sibling))
        if len(forwards) > 1:
            forwards[-2].wait_recv()
            expand_slot(order[len(forwards) - 2])
    if forwards:
        forwards[-1].wait_recv()
        expand_slot(order[-1])

    latent = ctxl[...].astype(BF16)
    rope_k = ctxr[...].T[:ROPE]
    up = nt_dot(wupt[...], latent)
    shared = jnp.sum(rope_k * rope_k, axis=0, keepdims=True)
    at = pl.ds(nlat, LANES)
    for h in range(2):
        part = up[h * HD : (h + 1) * HD]
        inv = lax.rsqrt((jnp.sum(part * part, axis=0, keepdims=True) + shared) * (1.0 / QK) + EPS)
        keys[h, h * HD : (h + 1) * HD, at] = (part * inv * kg[:HD]).astype(BF16)
        keys[h, LANES + h * ROPE : LANES + (h + 1) * ROPE, at] = (rope_k * inv * kg[HD:QK]).astype(BF16)
    value = jnp.dot(latent, wup[1], preferred_element_type=F32)
    low = lane_ids((LANES, LANES)) < HD
    real = row_ids((LANES, LANES)) < nz * crow
    ones = jnp.where(real, 1.0, 0.0)
    vals[0, at, :] = jnp.where(low, value, ones).astype(BF16)
    vals[1, at, :] = jnp.where(low, ones, value).astype(BF16)

    diagonal = lane_ids((LANES, LANES)) % HD == row_ids((LANES, LANES)) % HD

    low = lane_ids((LANES, LANES)) < HD
    late = lane_ids((1, nlat + LANES)) < nlat
    lifts = [jnp.where(late, lift_s[0, h] * LOG2E, 0.0) for h in range(2)]

    def whole_query(j):
        tails = qbuf[j, LANES:, :]
        turned_tails = pltpu.roll(tails.astype(F32), LANES // 2, 1).astype(BF16)
        return jnp.concatenate([qbuf[j, 0:LANES, :], jnp.concatenate([tails, turned_tails], axis=0)], axis=1)

    def attend(slots):
        q = jnp.concatenate([whole_query(j) for j in slots], axis=0)
        outs = []
        for h in range(2):
            p = jnp.exp2(jnp.dot(q, keys[h], preferred_element_type=F32) - lifts[h]).astype(BF16)
            outs.append(jnp.dot(p, vals[h], preferred_element_type=F32))
        for i, j in enumerate(slots):
            first, second = (out[i * LANES : (i + 1) * LANES] for out in outs)
            den = jnp.where(diagonal, jnp.where(low, second, first), 0.0)
            packed = jnp.concatenate(
                [
                    jnp.sum(den[:HD], axis=0, keepdims=True),
                    jnp.sum(den[HD:], axis=0, keepdims=True),
                ],
                axis=0,
            )
            hi = packed.astype(BF16).astype(F32)
            lo = packed - hi
            ostage[j, 0:LANES, :] = jnp.where(low, first, second).astype(BF16)
            ostage[j, LANES:, :] = jnp.concatenate([hi, lo, jnp.zeros((12, LANES), F32)], axis=0).astype(BF16)

    o_copies = []
    o_half = []
    halves = ((0, HD), (HD, ostage.shape[1] - HD))
    order = sorted(range(ny), key=lambda j: -min(j, ny - j))
    arrivals = {k: [q_near[k]] for k in direct(ny)}
    arrivals.update(q_far)
    arrivals[0] = []
    for at in range(0, ny, 2):
        slots = order[at : at + 2]
        for j in slots:
            landed(f for f in arrivals[j] if not f.landed)
        attend(slots)
        for j in slots:
            if j == 4:
                for side, step in ((0, 2), (1, ny - 2)):
                    rows_at = pl.ds(*halves[side])
                    o_half.append(
                        remote(ostage.at[j, rows_at, :], opass.at[rows_at, :], 138 + side, y_peer(step))
                    )
            elif j:
                o_copies.append(remote(ostage.at[j], obuf.at[j], 144 + j, y_peer(ny - j)))
    def pass_weights():
        for k in near_x:
            for flight in (w_first[k], w_second[k]):
                if not flight.landed:
                    flight.wait_recv()
            came = x_index(nx - k)
            w_side.append(remote(wout.at[came], wout.at[came], 175 + k, sibling))
        if w_far:
            landed(w_far)
            came = x_index(2)
            w_side.append(remote(wout.at[came], wout.at[came], 179, sibling))

    if o_half:
        for side, step in ((0, 2), (1, ny - 2)):
            o_half[side].wait_recv()
            rows_at = pl.ds(*halves[side])
            o_copies.append(remote(opass.at[rows_at, :], obuf.at[4, rows_at, :], 152 + side, y_peer(step)))
    pass_weights()
    landed(o_copies)
    num = ostage[0, 0:LANES, :].astype(F32)
    den = ostage[0, LANES:, :].astype(F32)
    for j in range(1, ny):
        num = num + obuf[j, 0:LANES, :].astype(F32)
        den = den + obuf[j, LANES:, :].astype(F32)
    den = den[0:2] + den[2:4]
    spread = jnp.concatenate(
        [
            jnp.broadcast_to(den[0:1], (HD, LANES)),
            jnp.broadcast_to(den[1:2], (HD, LANES)),
        ],
        axis=0,
    )
    spread = jnp.where(diagonal, spread, 0.0)
    swap = jnp.where((lane_ids((LANES, LANES)) < HD) != (row_ids((LANES, LANES)) < HD), 1.0, 0.0)
    spread = jnp.dot(spread, swap, precision=HIGHEST, preferred_element_type=F32)
    attended = (num / spread).astype(BF16)

    share_out[...] = attended.reshape(ntp, rows, LANES)
    heads[tp] = share_out[tp]
    a_copies = [
        remote(share_out.at[(tp + k) % ntp], heads.at[tp], 160 + k, t_peer(k)) for k in range(1, ntp)
    ]
    landed(w_side)
    landed(a_copies)
    mixed = jnp.concatenate([heads[t] for t in range(ntp)], axis=1)
    result = jnp.dot(mixed, wout[...].reshape(ntp * LANES, width), preferred_element_type=F32)
    landed(gt_copies)
    gate_row = jnp.concatenate([gtbuf[t] for t in range(ntp)], axis=1)
    out_ref[...] = (gtok[tp].astype(F32) + gate_row * result).astype(BF16)

    for flight in sent:
        flight.wait_send()


def solution(mesh, nz=8):
    nsp, ntp = mesh.shape["sp"], mesh.shape["tp"]
    ny = nsp // nz

    def local(
        latent_tokens,
        context_tokens,
        cond,
        ctx_cond,
        mod_shift,
        mod_scale,
        mod_gate,
        norm_gain,
        w_query,
        query_gain,
        w_down_kv,
        w_rope_key,
        kv_gain,
        w_up_kv,
        key_gain,
        ctx_lift,
        w_output,
    ):
        rows, width = latent_tokens.shape
        crow = context_tokens.shape[0]
        piece = mod_shift.shape[1]
        lat = nz * LANES
        vm = pltpu.VMEM
        anywhere = pl.BlockSpec(memory_space=pl.ANY)
        smem = pl.BlockSpec(memory_space=pltpu.SMEM)
        return pl.pallas_call(
            functools.partial(kernel, nz, ny, ntp),
            out_shape=jax.ShapeDtypeStruct((rows, width), BF16),
            in_specs=[anywhere] * 15 + [smem, anywhere],
            out_specs=pl.BlockSpec(memory_space=pltpu.VMEM),
            scratch_shapes=[
                vm((ntp, rows, width), BF16),
                vm((crow, width), BF16),
                vm((width // LANES, LANES), F32),
                vm((width // LANES, LANES), F32),
                vm((3, mod_shift.shape[0], piece), BF16),
                vm((1, width), F32),
                vm(w_query.shape[::-1], BF16),
                vm((1, QK), F32),
                vm(w_down_kv.shape, BF16),
                vm(w_rope_key.shape[::-1], BF16),
                vm((1, KVL), F32),
                vm(w_up_kv.shape, BF16),
                vm((1, QK), F32),
                vm((ntp, *w_output.shape), BF16),
                vm((nz, 2, 2 * piece), F32),
                vm((ny, 2, 2 * piece), F32),
                vm((ntp, 2, 2 * piece), F32),
                vm((nz, 1, piece), F32),
                vm((ny, 1, piece), F32),
                vm((ntp, 1, piece), F32),
                vm((LANES, width), F32),
                vm((crow, width), F32),
                vm((LANES + 16, width), BF16),
                vm((LANES, KVL), BF16),
                vm((nz, HALF, LANES), F32),
                vm((nz, HALF, LANES), F32),
                vm((nz, 2, MSG, KVL), BF16),
                vm((ny, LANES + HD, LANES), BF16),
                vm((2, 2 * LANES, lat + LANES), BF16),
                vm((2, lat + LANES, LANES), BF16),
                vm((LANES, KVL), F32),
                vm((LANES, LANES), F32),
                vm((ny, LANES + 16, LANES), BF16),
                vm((ny, LANES + 16, LANES), BF16),
                vm((LANES + 16, LANES), BF16),
                vm((ntp, rows, LANES), BF16),
                vm((ntp, rows, LANES), BF16),
                pltpu.SemaphoreType.DMA((16,)),
                pltpu.SemaphoreType.DMA((184,)),
                pltpu.SemaphoreType.DMA((184,)),
            ],
            compiler_params=pltpu.CompilerParams(
                collective_id=0, has_side_effects=True, vmem_limit_bytes=60 * 1024 * 1024
            ),
        )(
            latent_tokens,
            context_tokens,
            cond.reshape(width // LANES, LANES),
            ctx_cond.reshape(width // LANES, LANES),
            mod_shift,
            mod_scale,
            mod_gate,
            norm_gain.reshape(1, width),
            w_query.T,
            query_gain.reshape(1, QK),
            w_down_kv,
            w_rope_key.T,
            kv_gain.reshape(1, KVL),
            w_up_kv,
            key_gain.reshape(1, QK),
            ctx_lift.reshape(1, 2),
            w_output,
        )

    in_specs = (
        P(("sp", "tp"), None),
        P("sp", None),
        P(),
        P(),
        P("sp", "tp"),
        P("sp", "tp"),
        P("sp", "tp"),
        P(),
        P(None, "tp"),
        P(),
        P(),
        P(),
        P(),
        P(None, None, "tp"),
        P(),
        P("tp"),
        P("tp", None),
    )
    return jax.shard_map(local, mesh=mesh, in_specs=in_specs, out_specs=P(("sp", "tp"), None), check_vma=False)
```

```python
import functools
import math

import jax
import jax.numpy as jnp
from jax import lax
from jax.experimental import pallas as pl
from jax.experimental.pallas import tpu as pltpu
from jax.sharding import PartitionSpec as P

HD = 64
ROPE = 32
QK = 96
KVL = 256
HALF = ROPE // 2
GRID_W = 64
EPS = 1e-06
THETA = 10000.0
LOG2E = math.log2(math.e)
MESH = pl.DeviceIdType.MESH
F32 = jnp.float32
BF16 = jnp.bfloat16
HIGHEST = lax.Precision.HIGHEST
LANES = 128
MSG = 80


def nt_dot(a, b):
    return lax.dot_general(a, b, (((1,), (1,)), ((), ())), preferred_element_type=F32)


def lane_ids(shape):
    return lax.broadcasted_iota(jnp.int32, shape, 1)


def row_ids(shape):
    return lax.broadcasted_iota(jnp.int32, shape, 0)


def silu(v):
    return v / (1.0 + jnp.exp(-v))


def column_tile(row):
    width = row.shape[1]
    full = jnp.concatenate([row, jnp.zeros((1, LANES - width), F32)], axis=1)
    return jnp.broadcast_to(full, (LANES, LANES)).T


class Flight:
    def __init__(self, sent, copy):
        self.copy, self.landed = copy, False
        sent.append(self)
        copy.start()

    def wait_recv(self):
        self.landed = True
        self.copy.wait_recv()

    def wait_send(self):
        self.copy.wait_send()


def angle_tables(group):
    shape = (HALF, LANES)
    freq_row = row_ids(shape)
    token = lane_ids(shape)
    inverse = jnp.zeros(shape, F32)
    for j in range(HALF // 2):
        inverse = jnp.where(freq_row % (HALF // 2) == j, THETA ** (-j / (HALF // 2)), inverse)
    row = (group * (LANES // GRID_W) + token // GRID_W).astype(F32)
    col = (token % GRID_W).astype(F32)
    angle = jnp.where(freq_row < HALF // 2, row, col) * inverse
    return jnp.cos(angle), jnp.sin(angle)


def rotated(tail, cosine, sine):
    front, back = tail[:HALF], tail[HALF:]
    return jnp.concatenate([front * cosine - back * sine, back * cosine + front * sine], axis=0)


def kernel(
    nz,
    ny,
    ntp,
    tok_h,
    ctx_h,
    cond_h,
    cctx_h,
    mshift_h,
    mscale_h,
    mgate_h,
    ngain_h,
    wq_h,
    qgain_h,
    wdown_h,
    wrope_h,
    kvgain_h,
    wup_h,
    kgain_h,
    lift_s,
    wout_h,
    out_ref,
    gtok,
    ctok,
    cond_v,
    cctx_v,
    mods,
    ngain,
    wq,
    qgain,
    wdown,
    wrope,
    kvgain,
    wup,
    kgain,
    wout,
    zbuf,
    ybuf,
    tbuf,
    gzbuf,
    gybuf,
    gtbuf,
    nv,
    nvc,
    hid,
    wupt,
    ctab,
    stab,
    msg,
    qbuf,
    keys,
    vals,
    ctxl,
    ctxr,
    ostage,
    obuf,
    opass,
    osum,
    onext,
    share_out,
    heads,
    load_sem,
    send_sem,
    recv_sem,
):
    sp = lax.axis_index("sp")
    tp = lax.axis_index("tp")
    zi, yi = sp // ny, sp % ny
    core = tp % 2
    rows = tok_h.shape[0]
    width = tok_h.shape[1]
    piece = mods.shape[2]
    crow = ctx_h.shape[0]
    nlat = nz * LANES

    def z_peer(k):
        return (((zi + k) % nz) * ny + yi, tp)

    def y_peer(k):
        return (zi * ny + (yi + k) % ny, tp)

    def t_peer(k):
        return (sp, (tp + k) % ntp)

    sibling = (sp, tp + 1 - 2 * core)

    def x_index(k):
        return (tp + 2 * k) % ntp

    def x_peer(k):
        return (sp, x_index(k))

    pairs = [
        (cond_h, cond_v),
        (cctx_h, cctx_v),
        (mshift_h, mods.at[0]),
        (mscale_h, mods.at[1]),
        (mgate_h, mods.at[2]),
        (tok_h, gtok.at[tp]),
        (ctx_h, ctok),
        (ngain_h, ngain),
        (wup_h, wup),
        (kgain_h, kgain),
        (qgain_h, qgain),
        (kvgain_h, kvgain),
        (wdown_h, wdown),
        (wrope_h, wrope),
        (wq_h, wq),
        (wout_h, wout.at[tp]),
    ]
    loads = [pltpu.make_async_copy(a, b, load_sem.at[i]) for i, (a, b) in enumerate(pairs)]
    for copy in loads:
        copy.start()

    barrier = pltpu.get_barrier_semaphore()
    peers = (
        [z_peer(k) for k in range(1, nz)]
        + [y_peer(k) for k in range(1, ny)]
        + [t_peer(k) for k in range(1, ntp)]
    )
    for peer in peers:
        pl.semaphore_signal(barrier, inc=1, device_id=peer, device_id_type=MESH)

    for i in range(5):
        loads[i].wait()
    mod_rows = mods.shape[1]
    fold = LANES // mod_rows
    quarter = sp % fold
    own_row = sp // fold
    lat_row = silu(cond_v[pl.ds(own_row, 1), :])
    ctx_row = silu(cctx_v[pl.ds(own_row, 1), :])
    mine = lane_ids((1, LANES)) // mod_rows == quarter
    signal = jnp.concatenate(
        [jnp.where(mine, lat_row, 0.0), jnp.where(mine, ctx_row, 0.0), jnp.zeros((6, LANES), F32)],
        axis=0,
    )
    block = jnp.concatenate([mods[0], mods[1], mods[2]], axis=1).astype(F32)
    block = jnp.concatenate([block] * fold, axis=0)
    share = jnp.dot(signal, block, precision=HIGHEST, preferred_element_type=F32)
    zbuf[0] = share[0:2, : 2 * piece]
    gzbuf[0] = share[0:1, 2 * piece :]

    pl.semaphore_wait(barrier, len(peers))

    sent = []

    def remote(src, dst, index, device):
        return Flight(
            sent,
            pltpu.make_async_remote_copy(
                src_ref=src,
                dst_ref=dst,
                send_sem=send_sem.at[index],
                recv_sem=recv_sem.at[index],
                device_id=device,
                device_id_type=MESH,
            ),
        )

    def far_first(count):
        return sorted(range(1, count), key=lambda k: -min(k, count - k))

    def exchange(buf, count, peer, first):
        return [remote(buf.at[0], buf.at[k], first + k, peer(k)) for k in far_first(count)]

    def spread_tp(buf, first):
        return [remote(buf.at[tp], buf.at[tp], first + k, t_peer(k)) for k in range(1, ntp)]

    def direct(count):
        if count < 8:
            return list(range(1, count))
        return [2, count - 2, 1, count - 1]

    def landed(flights):
        for flight in flights:
            flight.wait_recv()

    z_copies = exchange(zbuf, nz, z_peer, 0)
    gz_copies = exchange(gzbuf, nz, z_peer, 8)

    loads[5].wait()
    near_x = sorted({k for k in (1, ntp // 2 - 1) if 0 < k < ntp // 2})
    tok_near = {k: remote(gtok.at[tp], gtok.at[tp], 16 + k, x_peer(k)) for k in near_x}
    tok_side = [remote(gtok.at[tp], gtok.at[tp], 16, sibling)]
    tok_half = []

    for i in range(6, 12):
        loads[i].wait()
    gain_row = ngain[...]
    cv = ctok[...].astype(F32)
    nvc[...] = cv * lax.rsqrt(jnp.mean(cv * cv, axis=1, keepdims=True) + EPS) * gain_row
    wupt[...] = wup[0].astype(F32).T.astype(BF16)
    keys[...] = jnp.zeros(keys.shape, BF16)
    vals[:, nlat:, :] = jnp.zeros((2, LANES, LANES), BF16)
    ctxl[...] = jnp.zeros(ctxl.shape, F32)
    ctxr[...] = jnp.zeros(ctxr.shape, F32)
    msg[0, :, 64:80, :] = jnp.zeros((2, 16, KVL), BF16)
    hid[LANES:, :] = jnp.zeros((hid.shape[0] - LANES, width), BF16)
    kg = column_tile(kgain[...])
    qg = column_tile(qgain[...]) * (LOG2E * QK ** (-0.5))
    for k in range(nz):
        cosine, sine = angle_tables(((zi + nz - k) % nz) * ny + yi)
        ctab[k] = cosine
        stab[k] = sine

    for k in near_x:
        tok_near[k].wait_recv()
        came = x_index(ntp // 2 - k)
        if ntp // 2 == 4:
            lanes = pl.ds(0 if k == 1 else width // 2, width // 2)
            tok_half.append(
                remote(gtok.at[came, :, lanes], gtok.at[came, :, lanes], 20 + k, x_peer(k))
            )
        tok_side.append(remote(gtok.at[came], gtok.at[came], 24 + k, sibling))

    nx = ntp // 2
    half_w = width // 2

    def columns(side):
        return pl.ds(side * half_w, half_w)

    def w_block(index, side):
        return wout.at[index, :, columns(side)]

    loads[15].wait()
    w_side = [remote(wout.at[tp], wout.at[tp], 168, sibling)]
    w_first = {k: remote(w_block(tp, side), w_block(tp, side), 169 + side, x_peer(k)) for side, k in enumerate(near_x)}

    landed(z_copies)
    total = zbuf[0]
    for k in range(1, nz):
        total = total + zbuf[k]
    ybuf[0] = total
    y_copies = exchange(ybuf, ny, y_peer, 32)
    landed(gz_copies)
    total = gzbuf[0]
    for k in range(1, nz):
        total = total + gzbuf[k]
    gybuf[0] = total
    gy_copies = exchange(gybuf, ny, y_peer, 40)

    if tok_half:
        landed(tok_half)
        far = x_index(2)
        tok_side.append(remote(gtok.at[far], gtok.at[far], 28, sibling))
    landed(y_copies)
    total = ybuf[0]
    for k in range(1, ny):
        total = total + ybuf[k]
    tbuf[tp] = total

    t_copies = spread_tp(tbuf, 48)
    landed(gy_copies)
    total = gybuf[0]
    for k in range(1, ny):
        total = total + gybuf[k]
    gtbuf[tp] = total
    gt_copies = spread_tp(gtbuf, 56)

    landed(tok_side)

    def norm_rows(i, carry):
        v = gtok[i].astype(F32)
        scaled = v * lax.rsqrt(jnp.mean(v * v, axis=1, keepdims=True) + EPS) * gain_row
        nv[pl.ds(pl.multiple_of(i * rows, rows), rows), :] = scaled
        return carry

    lax.fori_loop(0, ntp, norm_rows, 0)

    for i in range(12, 15):
        loads[i].wait()
    landed(t_copies)
    w_second = {k: remote(w_block(tp, 1 - side), w_block(tp, 1 - side), 171 + side, x_peer(k)) for side, k in enumerate(near_x)}
    w_far = []
    if nx == 4:
        for side, k in enumerate(near_x):
            w_first[k].wait_recv()
            came = x_index(nx - k)
            w_far.append(remote(w_block(came, side), w_block(came, side), 173 + side, x_peer(k)))

    def vector(which, who):
        return jnp.concatenate(
            [tbuf[t][who : who + 1, which * piece : (which + 1) * piece] for t in range(ntp)],
            axis=1,
        )

    shift_row = vector(0, 0)
    scale_row = 1.0 + vector(1, 0)

    def modulate(i, carry):
        at = pl.ds(pl.multiple_of(i * 16, 16), 16)
        hid[at, :] = (nv[at, :] * scale_row + shift_row).astype(BF16)
        return carry

    lax.fori_loop(0, LANES // 16, modulate, 0)
    ctx_hidden = nvc[...] * (1.0 + vector(1, 1)) + vector(0, 1)
    hid[LANES : LANES + 16, :] = jnp.concatenate(
        [ctx_hidden, jnp.zeros((16 - crow, width), F32)], axis=0
    ).astype(BF16)

    raw = jnp.dot(hid[...], wdown[...], preferred_element_type=F32)
    lat = raw * lax.rsqrt(jnp.mean(raw * raw, axis=1, keepdims=True) + EPS) * kvgain[...]
    rope_t = nt_dot(wrope[...], hid[:LANES, :])
    rope_c = nt_dot(hid[LANES:, :], wrope[...])
    rope_c = jnp.concatenate([rope_c, jnp.zeros((16, LANES - ROPE), F32)], axis=1)
    ctx_lat = lat[LANES : LANES + crow]
    msg[0, 0, 0:64, :] = lat[0:64].astype(BF16)
    msg[0, 1, 0:64, :] = lat[64:128].astype(BF16)
    msg[0, 0, 64:80, 0:LANES] = rope_t[:16].astype(BF16)
    msg[0, 1, 64:80, 0:LANES] = rope_t[16:].astype(BF16)
    msg[0, 0, 64:80, LANES:] = jnp.concatenate([ctx_lat[:, :LANES], ctx_lat[:, LANES:]], axis=0).astype(BF16)
    msg[0, 1, 64:80, LANES:] = rope_c.astype(BF16)
    k_near = {
        k: remote(msg.at[0, core], msg.at[k, core], 64 + k, z_peer(k)) for k in direct(nz)
    }

    raw_t = nt_dot(wq[...], hid[:LANES, :])
    plains, tails = [], []
    for h in range(2):
        u = raw_t[h * QK : (h + 1) * QK]
        inv = lax.rsqrt(jnp.sum(u * u, axis=0, keepdims=True) * (1.0 / QK) + EPS)
        u = u * inv * qg[:QK]
        plains.append(u[:HD])
        tails.append(rotated(u[HD:], ctab[0], stab[0]))
    plain = jnp.concatenate(plains, axis=0).T
    tail = jnp.concatenate(tails, axis=0)
    tail = jnp.concatenate([tail, pltpu.roll(tail, LANES // 2, 1)], axis=0).T
    qbuf[0, 0:LANES, :] = plain.astype(BF16)
    qbuf[0, LANES:, :] = tail[: LANES // 2].astype(BF16)
    q_near = {k: remote(qbuf.at[0], qbuf.at[k], 80 + k, y_peer(k)) for k in direct(ny)}

    def expand_slot(k):
        latent = msg[k, :, 0:64, :].reshape(LANES, KVL)
        rope_k = jnp.concatenate([msg[k, 0, 64:80, 0:LANES], msg[k, 1, 64:80, 0:LANES]], axis=0).astype(F32)
        up = nt_dot(wupt[...], latent)
        shared = jnp.sum(rope_k * rope_k, axis=0, keepdims=True)
        at = pl.ds(k * LANES, LANES)
        for h in range(2):
            part = up[h * HD : (h + 1) * HD]
            inv = lax.rsqrt((jnp.sum(part * part, axis=0, keepdims=True) + shared) * (1.0 / QK) + EPS)
            keys[h, h * HD : (h + 1) * HD, at] = (part * inv * kg[:HD]).astype(BF16)
            turned = rotated(rope_k * inv * kg[HD:QK], ctab[k], stab[k])
            keys[h, LANES + h * ROPE : LANES + (h + 1) * ROPE, at] = turned.astype(BF16)
        value = jnp.dot(latent, wup[1], preferred_element_type=F32)
        low = lane_ids((LANES, LANES)) < HD
        vals[0, at, :] = jnp.where(low, value, 1.0).astype(BF16)
        vals[1, at, :] = jnp.where(low, 1.0, value).astype(BF16)
        ctx_two = msg[k, 0, 64:80, LANES:].astype(F32)
        ctxl[k * crow : (k + 1) * crow, :] = jnp.concatenate([ctx_two[:crow], ctx_two[8 : 8 + crow]], axis=1)
        ctxr[k * crow : (k + 1) * crow, :] = msg[k, 1, 64:80, LANES:].astype(F32)[:crow]

    expand_slot(0)
    def relay(near, buf, whole, part, count, peer, first):
        if count < 8:
            return {}
        for k in (2, count - 2):
            near[k].wait_recv()
        out = {count // 2: []}
        for side, k, step in ((0, 2, 1), (1, count - 2, count - 1)):
            onward = (k + step) % count
            out[onward] = [remote(whole(buf.at[k]), whole(buf.at[onward]), first + onward, peer(step))]
        for side, k in ((0, 2), (1, count - 2)):
            out[count // 2].append(
                remote(part(buf.at[k], side), part(buf.at[count // 2], side), first + 8 + side, peer(k))
            )
        return out

    def key_whole(ref):
        return ref.at[core]

    def key_part(ref, side):
        return ref.at[core, :, pl.ds(side * LANES, LANES)]

    def query_whole(ref):
        return ref

    def query_part(ref, side):
        return ref.at[pl.ds(side * (qrows // 2), qrows // 2), :]

    qrows = qbuf.shape[1]
    k_far = relay(k_near, msg, key_whole, key_part, nz, z_peer, 96)
    q_far = relay(q_near, qbuf, query_whole, query_part, ny, y_peer, 112)
    arrivals = {k: [k_near[k]] for k in direct(nz)}
    arrivals.update(k_far)
    forwards = []
    order = direct(nz) + sorted(k_far, key=lambda k: min(k, nz - k))
    for k in order:
        landed(f for f in arrivals[k] if not f.landed)
        forwards.append(remote(msg.at[k, core], msg.at[k, core], 128 + k, sibling))
        if len(forwards) > 1:
            forwards[-2].wait_recv()
            expand_slot(order[len(forwards) - 2])
    if forwards:
        forwards[-1].wait_recv()
        expand_slot(order[-1])

    latent = ctxl[...].astype(BF16)
    rope_k = ctxr[...].T[:ROPE]
    up = nt_dot(wupt[...], latent)
    shared = jnp.sum(rope_k * rope_k, axis=0, keepdims=True)
    at = pl.ds(nlat, LANES)
    for h in range(2):
        part = up[h * HD : (h + 1) * HD]
        inv = lax.rsqrt((jnp.sum(part * part, axis=0, keepdims=True) + shared) * (1.0 / QK) + EPS)
        keys[h, h * HD : (h + 1) * HD, at] = (part * inv * kg[:HD]).astype(BF16)
        keys[h, LANES + h * ROPE : LANES + (h + 1) * ROPE, at] = (rope_k * inv * kg[HD:QK]).astype(BF16)
    value = jnp.dot(latent, wup[1], preferred_element_type=F32)
    low = lane_ids((LANES, LANES)) < HD
    real = row_ids((LANES, LANES)) < nz * crow
    ones = jnp.where(real, 1.0, 0.0)
    vals[0, at, :] = jnp.where(low, value, ones).astype(BF16)
    vals[1, at, :] = jnp.where(low, ones, value).astype(BF16)

    diagonal = lane_ids((LANES, LANES)) % HD == row_ids((LANES, LANES)) % HD

    low = lane_ids((LANES, LANES)) < HD
    late = lane_ids((1, nlat + LANES)) < nlat
    lifts = [jnp.where(late, lift_s[0, h] * LOG2E, 0.0) for h in range(2)]

    def whole_query(j):
        tails = qbuf[j, LANES:, :]
        turned_tails = pltpu.roll(tails.astype(F32), LANES // 2, 1).astype(BF16)
        return jnp.concatenate([qbuf[j, 0:LANES, :], jnp.concatenate([tails, turned_tails], axis=0)], axis=1)

    def attend(slots):
        q = jnp.concatenate([whole_query(j) for j in slots], axis=0)
        outs = []
        for h in range(2):
            p = jnp.exp2(jnp.dot(q, keys[h], preferred_element_type=F32) - lifts[h]).astype(BF16)
            outs.append(jnp.dot(p, vals[h], preferred_element_type=F32))
        for i, j in enumerate(slots):
            first, second = (out[i * LANES : (i + 1) * LANES] for out in outs)
            den = jnp.where(diagonal, jnp.where(low, second, first), 0.0)
            packed = jnp.concatenate(
                [
                    jnp.sum(den[:HD], axis=0, keepdims=True),
                    jnp.sum(den[HD:], axis=0, keepdims=True),
                ],
                axis=0,
            )
            hi = packed.astype(BF16).astype(F32)
            lo = packed - hi
            ostage[j, 0:LANES, :] = jnp.where(low, first, second).astype(BF16)
            ostage[j, LANES:, :] = jnp.concatenate([hi, lo, jnp.zeros((12, LANES), F32)], axis=0).astype(BF16)

    def packed_rows(ref):
        block = ref[...].astype(F32)
        return block[:LANES], block[LANES : LANES + 2] + block[LANES + 2 : LANES + 4]

    def store_packed(ref, num, den):
        hi = den.astype(BF16).astype(F32)
        ref[0:LANES, :] = num.astype(BF16)
        ref[LANES:, :] = jnp.concatenate([hi, den - hi, jnp.zeros((12, LANES), F32)], axis=0).astype(BF16)

    o_copies = []
    o_add = {}
    halves = ((0, HD), (HD, ostage.shape[1] - HD))
    arrivals = {k: [q_near[k]] for k in direct(ny)}
    arrivals.update(q_far)
    arrivals[0] = []
    joined = ny >= 8
    if joined:
        order = [3, ny - 3, ny // 2, 0, 2, ny - 2, 1, ny - 1]
    else:
        order = sorted(range(ny), key=lambda j: -min(j, ny - j))
    for at in range(0, ny, 2):
        slots = order[at : at + 2]
        for j in slots:
            landed(f for f in arrivals[j] if not f.landed)
        attend(slots)
        for j in slots:
            if j == 0 or (joined and j in (2, ny - 2)):
                continue
            if joined and j in (3, ny - 3):
                side = 0 if j == 3 else 1
                o_add[side] = [remote(ostage.at[j], osum.at[side], 138 + side, y_peer(ny - 1 if side == 0 else 1))]
            elif joined and j == ny // 2:
                for side in range(2):
                    rows_at = pl.ds(*halves[side])
                    o_add[side].append(
                        remote(
                            ostage.at[j, rows_at, :],
                            opass.at[rows_at, :],
                            140 + side,
                            y_peer(ny - 2 if side == 0 else 2),
                        )
                    )
            else:
                o_copies.append(remote(ostage.at[j], obuf.at[j], 144 + j, y_peer(ny - j)))
    if joined:
        for side in range(2):
            landed(o_add[side])
        passed_num, passed_den = packed_rows(opass)
        for side, j in ((0, 2), (1, ny - 2)):
            num, den = packed_rows(ostage.at[j])
            more_num, more_den = packed_rows(osum.at[side])
            blank = jnp.zeros((HD, LANES), F32)
            if side == 0:
                extra = jnp.concatenate([passed_num[:HD], blank], axis=0)
            else:
                extra = jnp.concatenate([blank, passed_num[HD:]], axis=0)
                more_den = more_den + passed_den
            store_packed(onext.at[side], num + more_num + extra, den + more_den)
            o_copies.append(remote(onext.at[side], obuf.at[j], 144 + j, y_peer(ny - j)))
    sources = [k for k in range(1, ny) if not joined or k in (1, 2, ny - 2, ny - 1)]

    def pass_weights():
        for k in near_x:
            for flight in (w_first[k], w_second[k]):
                if not flight.landed:
                    flight.wait_recv()
            came = x_index(nx - k)
            w_side.append(remote(wout.at[came], wout.at[came], 175 + k, sibling))
        if w_far:
            landed(w_far)
            came = x_index(2)
            w_side.append(remote(wout.at[came], wout.at[came], 179, sibling))

    pass_weights()
    landed(o_copies)
    num = ostage[0, 0:LANES, :].astype(F32)
    den = ostage[0, LANES:, :].astype(F32)
    for j in sources:
        num = num + obuf[j, 0:LANES, :].astype(F32)
        den = den + obuf[j, LANES:, :].astype(F32)
    den = den[0:2] + den[2:4]
    spread = jnp.concatenate(
        [
            jnp.broadcast_to(den[0:1], (HD, LANES)),
            jnp.broadcast_to(den[1:2], (HD, LANES)),
        ],
        axis=0,
    )
    spread = jnp.where(diagonal, spread, 0.0)
    swap = jnp.where((lane_ids((LANES, LANES)) < HD) != (row_ids((LANES, LANES)) < HD), 1.0, 0.0)
    spread = jnp.dot(spread, swap, precision=HIGHEST, preferred_element_type=F32)
    attended = (num / spread).astype(BF16)

    share_out[...] = attended.reshape(ntp, rows, LANES)
    heads[tp] = share_out[tp]
    a_copies = [
        remote(share_out.at[(tp + k) % ntp], heads.at[tp], 160 + k, t_peer(k)) for k in range(1, ntp)
    ]
    landed(w_side)
    landed(a_copies)
    mixed = jnp.concatenate([heads[t] for t in range(ntp)], axis=1)
    result = jnp.dot(mixed, wout[...].reshape(ntp * LANES, width), preferred_element_type=F32)
    landed(gt_copies)
    gate_row = jnp.concatenate([gtbuf[t] for t in range(ntp)], axis=1)
    out_ref[...] = gate_row * result

    for flight in sent:
        flight.wait_send()


def solution(mesh, nz=8):
    nsp, ntp = mesh.shape["sp"], mesh.shape["tp"]
    ny = nsp // nz

    def local(
        latent_tokens,
        context_tokens,
        cond,
        ctx_cond,
        mod_shift,
        mod_scale,
        mod_gate,
        norm_gain,
        w_query,
        query_gain,
        w_down_kv,
        w_rope_key,
        kv_gain,
        w_up_kv,
        key_gain,
        ctx_lift,
        w_output,
    ):
        rows, width = latent_tokens.shape
        crow = context_tokens.shape[0]
        piece = mod_shift.shape[1]
        lat = nz * LANES
        vm = pltpu.VMEM
        anywhere = pl.BlockSpec(memory_space=pl.ANY)
        smem = pl.BlockSpec(memory_space=pltpu.SMEM)
        update = pl.pallas_call(
            functools.partial(kernel, nz, ny, ntp),
            out_shape=jax.ShapeDtypeStruct((rows, width), F32),
            in_specs=[anywhere] * 15 + [smem, anywhere],
            out_specs=pl.BlockSpec(memory_space=pltpu.VMEM),
            scratch_shapes=[
                vm((ntp, rows, width), BF16),
                vm((crow, width), BF16),
                vm((width // LANES, LANES), F32),
                vm((width // LANES, LANES), F32),
                vm((3, mod_shift.shape[0], piece), BF16),
                vm((1, width), F32),
                vm(w_query.shape[::-1], BF16),
                vm((1, QK), F32),
                vm(w_down_kv.shape, BF16),
                vm(w_rope_key.shape[::-1], BF16),
                vm((1, KVL), F32),
                vm(w_up_kv.shape, BF16),
                vm((1, QK), F32),
                vm((ntp, *w_output.shape), BF16),
                vm((nz, 2, 2 * piece), F32),
                vm((ny, 2, 2 * piece), F32),
                vm((ntp, 2, 2 * piece), F32),
                vm((nz, 1, piece), F32),
                vm((ny, 1, piece), F32),
                vm((ntp, 1, piece), F32),
                vm((LANES, width), F32),
                vm((crow, width), F32),
                vm((LANES + 16, width), BF16),
                vm((LANES, KVL), BF16),
                vm((nz, HALF, LANES), F32),
                vm((nz, HALF, LANES), F32),
                vm((nz, 2, MSG, KVL), BF16),
                vm((ny, LANES + HD, LANES), BF16),
                vm((2, 2 * LANES, lat + LANES), BF16),
                vm((2, lat + LANES, LANES), BF16),
                vm((LANES, KVL), F32),
                vm((LANES, LANES), F32),
                vm((ny, LANES + 16, LANES), BF16),
                vm((ny, LANES + 16, LANES), BF16),
                vm((LANES + 16, LANES), BF16),
                vm((2, LANES + 16, LANES), BF16),
                vm((2, LANES + 16, LANES), BF16),
                vm((ntp, rows, LANES), BF16),
                vm((ntp, rows, LANES), BF16),
                pltpu.SemaphoreType.DMA((16,)),
                pltpu.SemaphoreType.DMA((184,)),
                pltpu.SemaphoreType.DMA((184,)),
            ],
            compiler_params=pltpu.CompilerParams(
                collective_id=0, has_side_effects=True, vmem_limit_bytes=60 * 1024 * 1024
            ),
        )(
            latent_tokens,
            context_tokens,
            cond.reshape(width // LANES, LANES),
            ctx_cond.reshape(width // LANES, LANES),
            mod_shift,
            mod_scale,
            mod_gate,
            norm_gain.reshape(1, width),
            w_query.T,
            query_gain.reshape(1, QK),
            w_down_kv,
            w_rope_key.T,
            kv_gain.reshape(1, KVL),
            w_up_kv,
            key_gain.reshape(1, QK),
            ctx_lift.reshape(1, 2),
            w_output,
        )
        return (latent_tokens.astype(F32) + update).astype(BF16)

    in_specs = (
        P(("sp", "tp"), None),
        P("sp", None),
        P(),
        P(),
        P("sp", "tp"),
        P("sp", "tp"),
        P("sp", "tp"),
        P(),
        P(None, "tp"),
        P(),
        P(),
        P(),
        P(),
        P(None, None, "tp"),
        P(),
        P("tp"),
        P("tp", None),
    )
    return jax.shard_map(local, mesh=mesh, in_specs=in_specs, out_specs=P(("sp", "tp"), None), check_vma=False)
```

```python
import functools
import math

import jax
import jax.numpy as jnp
from jax import lax
from jax.experimental import pallas as pl
from jax.experimental.pallas import tpu as pltpu
from jax.sharding import PartitionSpec as P

HD = 64
ROPE = 32
QK = 96
KVL = 256
HALF = ROPE // 2
GRID_W = 64
EPS = 1e-06
THETA = 10000.0
LOG2E = math.log2(math.e)
MESH = pl.DeviceIdType.MESH
F32 = jnp.float32
BF16 = jnp.bfloat16
HIGHEST = lax.Precision.HIGHEST
LANES = 128
MSG = 80


def nt_dot(a, b):
    return lax.dot_general(a, b, (((1,), (1,)), ((), ())), preferred_element_type=F32)


def lane_ids(shape):
    return lax.broadcasted_iota(jnp.int32, shape, 1)


def row_ids(shape):
    return lax.broadcasted_iota(jnp.int32, shape, 0)


def silu(v):
    return v / (1.0 + jnp.exp(-v))


def column_tile(row):
    width = row.shape[1]
    full = jnp.concatenate([row, jnp.zeros((1, LANES - width), F32)], axis=1)
    return jnp.broadcast_to(full, (LANES, LANES)).T


class Flight:
    def __init__(self, sent, copy):
        self.copy, self.landed = copy, False
        sent.append(self)
        copy.start()

    def wait_recv(self):
        self.landed = True
        self.copy.wait_recv()

    def wait_send(self):
        self.copy.wait_send()


def angle_tables(group):
    shape = (HALF, LANES)
    freq_row = row_ids(shape)
    token = lane_ids(shape)
    inverse = jnp.zeros(shape, F32)
    for j in range(HALF // 2):
        inverse = jnp.where(freq_row % (HALF // 2) == j, THETA ** (-j / (HALF // 2)), inverse)
    row = (group * (LANES // GRID_W) + token // GRID_W).astype(F32)
    col = (token % GRID_W).astype(F32)
    angle = jnp.where(freq_row < HALF // 2, row, col) * inverse
    return jnp.cos(angle), jnp.sin(angle)


def rotated(tail, cosine, sine):
    front, back = tail[:HALF], tail[HALF:]
    return jnp.concatenate([front * cosine - back * sine, back * cosine + front * sine], axis=0)


def kernel(
    nz,
    ny,
    ntp,
    tok_h,
    ctx_h,
    cond_h,
    cctx_h,
    mshift_h,
    mscale_h,
    mgate_h,
    ngain_h,
    wq_h,
    qgain_h,
    wdown_h,
    wrope_h,
    kvgain_h,
    wup_h,
    kgain_h,
    lift_s,
    wout_h,
    out_ref,
    gtok,
    ctok,
    cond_v,
    cctx_v,
    mods,
    ngain,
    wq,
    qgain,
    wdown,
    wrope,
    kvgain,
    wup,
    kgain,
    wout,
    zbuf,
    ybuf,
    tbuf,
    gzbuf,
    gybuf,
    gtbuf,
    nv,
    nvc,
    hid,
    wupt,
    ctab,
    stab,
    msg,
    qbuf,
    keys,
    vals,
    near_sum,
    ctxl,
    ctxr,
    ostage,
    obuf,
    opass,
    share_out,
    heads,
    load_sem,
    send_sem,
    recv_sem,
):
    sp = lax.axis_index("sp")
    tp = lax.axis_index("tp")
    zi, yi = sp // ny, sp % ny
    core = tp % 2
    rows = tok_h.shape[0]
    width = tok_h.shape[1]
    piece = mods.shape[2]
    crow = ctx_h.shape[0]
    nlat = nz * LANES

    def z_peer(k):
        return (((zi + k) % nz) * ny + yi, tp)

    def y_peer(k):
        return (zi * ny + (yi + k) % ny, tp)

    def t_peer(k):
        return (sp, (tp + k) % ntp)

    sibling = (sp, tp + 1 - 2 * core)

    def x_index(k):
        return (tp + 2 * k) % ntp

    def x_peer(k):
        return (sp, x_index(k))

    pairs = [
        (cond_h, cond_v),
        (cctx_h, cctx_v),
        (mshift_h, mods.at[0]),
        (mscale_h, mods.at[1]),
        (mgate_h, mods.at[2]),
        (tok_h, gtok.at[tp]),
        (ctx_h, ctok),
        (ngain_h, ngain),
        (wup_h, wup),
        (kgain_h, kgain),
        (qgain_h, qgain),
        (kvgain_h, kvgain),
        (wdown_h, wdown),
        (wrope_h, wrope),
        (wq_h, wq),
        (wout_h, wout.at[tp]),
    ]
    loads = [pltpu.make_async_copy(a, b, load_sem.at[i]) for i, (a, b) in enumerate(pairs)]
    for copy in loads:
        copy.start()

    barrier = pltpu.get_barrier_semaphore()
    peers = (
        [z_peer(k) for k in range(1, nz)]
        + [y_peer(k) for k in range(1, ny)]
        + [t_peer(k) for k in range(1, ntp)]
    )
    for peer in peers:
        pl.semaphore_signal(barrier, inc=1, device_id=peer, device_id_type=MESH)

    for i in range(5):
        loads[i].wait()
    mod_rows = mods.shape[1]
    fold = LANES // mod_rows
    quarter = sp % fold
    own_row = sp // fold
    lat_row = silu(cond_v[pl.ds(own_row, 1), :])
    ctx_row = silu(cctx_v[pl.ds(own_row, 1), :])
    mine = lane_ids((1, LANES)) // mod_rows == quarter
    signal = jnp.concatenate(
        [jnp.where(mine, lat_row, 0.0), jnp.where(mine, ctx_row, 0.0), jnp.zeros((6, LANES), F32)],
        axis=0,
    )
    block = jnp.concatenate([mods[0], mods[1], mods[2]], axis=1).astype(F32)
    block = jnp.concatenate([block] * fold, axis=0)
    share = jnp.dot(signal, block, precision=HIGHEST, preferred_element_type=F32)
    zbuf[0] = share[0:2, : 2 * piece]
    gzbuf[0] = share[0:1, 2 * piece :]

    pl.semaphore_wait(barrier, len(peers))

    sent = []

    def remote(src, dst, index, device):
        return Flight(
            sent,
            pltpu.make_async_remote_copy(
                src_ref=src,
                dst_ref=dst,
                send_sem=send_sem.at[index],
                recv_sem=recv_sem.at[index],
                device_id=device,
                device_id_type=MESH,
            ),
        )

    def far_first(count):
        return sorted(range(1, count), key=lambda k: -min(k, count - k))

    def exchange(buf, count, peer, first):
        return [remote(buf.at[0], buf.at[k], first + k, peer(k)) for k in far_first(count)]

    def spread_tp(buf, first):
        return [remote(buf.at[tp], buf.at[tp], first + k, t_peer(k)) for k in range(1, ntp)]

    def direct(count):
        if count < 8:
            return list(range(1, count))
        return [2, count - 2, 1, count - 1]

    def landed(flights):
        for flight in flights:
            flight.wait_recv()

    z_copies = exchange(zbuf, nz, z_peer, 0)
    gz_copies = exchange(gzbuf, nz, z_peer, 8)

    loads[5].wait()
    near_x = sorted({k for k in (1, ntp // 2 - 1) if 0 < k < ntp // 2})
    tok_near = {k: remote(gtok.at[tp], gtok.at[tp], 16 + k, x_peer(k)) for k in near_x}
    tok_side = [remote(gtok.at[tp], gtok.at[tp], 16, sibling)]
    tok_half = []

    for i in range(6, 12):
        loads[i].wait()
    gain_row = ngain[...]
    cv = ctok[...].astype(F32)
    nvc[...] = cv * lax.rsqrt(jnp.mean(cv * cv, axis=1, keepdims=True) + EPS) * gain_row
    wupt[...] = wup[0].astype(F32).T.astype(BF16)
    keys[...] = jnp.zeros(keys.shape, BF16)
    vals[:, nlat:, :] = jnp.zeros((2, LANES, LANES), BF16)
    ctxl[...] = jnp.zeros(ctxl.shape, F32)
    ctxr[...] = jnp.zeros(ctxr.shape, F32)
    msg[0, :, 64:80, :] = jnp.zeros((2, 16, KVL), BF16)
    hid[LANES:, :] = jnp.zeros((hid.shape[0] - LANES, width), BF16)
    kg = column_tile(kgain[...])
    qg = column_tile(qgain[...]) * (LOG2E * QK ** (-0.5))
    for k in range(nz):
        cosine, sine = angle_tables(((zi + nz - k) % nz) * ny + yi)
        ctab[k] = cosine
        stab[k] = sine

    for k in near_x:
        tok_near[k].wait_recv()
        came = x_index(ntp // 2 - k)
        if ntp // 2 == 4:
            lanes = pl.ds(0 if k == 1 else width // 2, width // 2)
            tok_half.append(
                remote(gtok.at[came, :, lanes], gtok.at[came, :, lanes], 20 + k, x_peer(k))
            )
        tok_side.append(remote(gtok.at[came], gtok.at[came], 24 + k, sibling))

    nx = ntp // 2
    half_w = width // 2

    def columns(side):
        return pl.ds(side * half_w, half_w)

    def w_block(index, side):
        return wout.at[index, :, columns(side)]

    loads[15].wait()
    w_side = [remote(wout.at[tp], wout.at[tp], 168, sibling)]
    w_first = {k: remote(w_block(tp, side), w_block(tp, side), 169 + side, x_peer(k)) for side, k in enumerate(near_x)}

    landed(z_copies)
    total = zbuf[0]
    for k in range(1, nz):
        total = total + zbuf[k]
    ybuf[0] = total
    y_copies = exchange(ybuf, ny, y_peer, 32)
    landed(gz_copies)
    total = gzbuf[0]
    for k in range(1, nz):
        total = total + gzbuf[k]
    gybuf[0] = total
    gy_copies = exchange(gybuf, ny, y_peer, 40)

    if tok_half:
        landed(tok_half)
        far = x_index(2)
        tok_side.append(remote(gtok.at[far], gtok.at[far], 28, sibling))
    landed(y_copies)
    total = ybuf[0]
    for k in range(1, ny):
        total = total + ybuf[k]
    tbuf[tp] = total

    t_copies = spread_tp(tbuf, 48)
    landed(gy_copies)
    total = gybuf[0]
    for k in range(1, ny):
        total = total + gybuf[k]
    gtbuf[tp] = total
    gt_copies = spread_tp(gtbuf, 56)

    landed(tok_side)

    def norm_rows(i, carry):
        v = gtok[i].astype(F32)
        scaled = v * lax.rsqrt(jnp.mean(v * v, axis=1, keepdims=True) + EPS) * gain_row
        nv[pl.ds(pl.multiple_of(i * rows, rows), rows), :] = scaled
        return carry

    lax.fori_loop(0, ntp, norm_rows, 0)

    for i in range(12, 15):
        loads[i].wait()
    landed(t_copies)
    w_second = {k: remote(w_block(tp, 1 - side), w_block(tp, 1 - side), 171 + side, x_peer(k)) for side, k in enumerate(near_x)}
    w_far = []
    if nx == 4:
        for side, k in enumerate(near_x):
            w_first[k].wait_recv()
            came = x_index(nx - k)
            w_far.append(remote(w_block(came, side), w_block(came, side), 173 + side, x_peer(k)))

    def vector(which, who):
        return jnp.concatenate(
            [tbuf[t][who : who + 1, which * piece : (which + 1) * piece] for t in range(ntp)],
            axis=1,
        )

    shift_row = vector(0, 0)
    scale_row = 1.0 + vector(1, 0)

    def modulate(i, carry):
        at = pl.ds(pl.multiple_of(i * 16, 16), 16)
        hid[at, :] = (nv[at, :] * scale_row + shift_row).astype(BF16)
        return carry

    lax.fori_loop(0, LANES // 16, modulate, 0)
    ctx_hidden = nvc[...] * (1.0 + vector(1, 1)) + vector(0, 1)
    hid[LANES : LANES + 16, :] = jnp.concatenate(
        [ctx_hidden, jnp.zeros((16 - crow, width), F32)], axis=0
    ).astype(BF16)

    raw = jnp.dot(hid[...], wdown[...], preferred_element_type=F32)
    lat = raw * lax.rsqrt(jnp.mean(raw * raw, axis=1, keepdims=True) + EPS) * kvgain[...]
    rope_t = nt_dot(wrope[...], hid[:LANES, :])
    rope_c = nt_dot(hid[LANES:, :], wrope[...])
    rope_c = jnp.concatenate([rope_c, jnp.zeros((16, LANES - ROPE), F32)], axis=1)
    ctx_lat = lat[LANES : LANES + crow]
    msg[0, 0, 0:64, :] = lat[0:64].astype(BF16)
    msg[0, 1, 0:64, :] = lat[64:128].astype(BF16)
    msg[0, 0, 64:80, 0:LANES] = rope_t[:16].astype(BF16)
    msg[0, 1, 64:80, 0:LANES] = rope_t[16:].astype(BF16)
    msg[0, 0, 64:80, LANES:] = jnp.concatenate([ctx_lat[:, :LANES], ctx_lat[:, LANES:]], axis=0).astype(BF16)
    msg[0, 1, 64:80, LANES:] = rope_c.astype(BF16)
    k_near = {
        k: remote(msg.at[0, core], msg.at[k, core], 64 + k, z_peer(k)) for k in direct(nz)
    }

    raw_t = nt_dot(wq[...], hid[:LANES, :])
    plains, tails = [], []
    for h in range(2):
        u = raw_t[h * QK : (h + 1) * QK]
        inv = lax.rsqrt(jnp.sum(u * u, axis=0, keepdims=True) * (1.0 / QK) + EPS)
        u = u * inv * qg[:QK]
        plains.append(u[:HD])
        tails.append(rotated(u[HD:], ctab[0], stab[0]))
    plain = jnp.concatenate(plains, axis=0).T
    tail = jnp.concatenate(tails, axis=0)
    tail = jnp.concatenate([tail, pltpu.roll(tail, LANES // 2, 1)], axis=0).T
    qbuf[0, 0:LANES, :] = plain.astype(BF16)
    qbuf[0, LANES:, :] = tail[: LANES // 2].astype(BF16)
    q_near = {k: remote(qbuf.at[0], qbuf.at[k], 80 + k, y_peer(k)) for k in direct(ny)}

    place = {k: at for at, k in enumerate([0] + direct(nz) + [k for k in range(1, nz) if k not in direct(nz)])}
    near_keys = (1 + len(direct(nz))) * LANES

    def expand_slot(k):
        latent = msg[k, :, 0:64, :].reshape(LANES, KVL)
        rope_k = jnp.concatenate([msg[k, 0, 64:80, 0:LANES], msg[k, 1, 64:80, 0:LANES]], axis=0).astype(F32)
        up = nt_dot(wupt[...], latent)
        shared = jnp.sum(rope_k * rope_k, axis=0, keepdims=True)
        at = pl.ds(place[k] * LANES, LANES)
        for h in range(2):
            part = up[h * HD : (h + 1) * HD]
            inv = lax.rsqrt((jnp.sum(part * part, axis=0, keepdims=True) + shared) * (1.0 / QK) + EPS)
            keys[h, h * HD : (h + 1) * HD, at] = (part * inv * kg[:HD]).astype(BF16)
            turned = rotated(rope_k * inv * kg[HD:QK], ctab[k], stab[k])
            keys[h, LANES + h * ROPE : LANES + (h + 1) * ROPE, at] = turned.astype(BF16)
        value = jnp.dot(latent, wup[1], preferred_element_type=F32)
        low = lane_ids((LANES, LANES)) < HD
        vals[0, at, :] = jnp.where(low, value, 1.0).astype(BF16)
        vals[1, at, :] = jnp.where(low, 1.0, value).astype(BF16)
        ctx_two = msg[k, 0, 64:80, LANES:].astype(F32)
        ctxl[k * crow : (k + 1) * crow, :] = jnp.concatenate([ctx_two[:crow], ctx_two[8 : 8 + crow]], axis=1)
        ctxr[k * crow : (k + 1) * crow, :] = msg[k, 1, 64:80, LANES:].astype(F32)[:crow]

    diagonal = lane_ids((LANES, LANES)) % HD == row_ids((LANES, LANES)) % HD
    low = lane_ids((LANES, LANES)) < HD
    late = lane_ids((1, nlat + LANES)) < nlat
    lifts = [jnp.where(late, lift_s[0, h] * LOG2E, 0.0) for h in range(2)]

    def whole_query(j):
        tails = qbuf[j, LANES:, :]
        turned_tails = pltpu.roll(tails.astype(F32), LANES // 2, 1).astype(BF16)
        return jnp.concatenate([qbuf[j, 0:LANES, :], jnp.concatenate([tails, turned_tails], axis=0)], axis=1)

    def mix(slots, start, stop):
        q = jnp.concatenate([whole_query(j) for j in slots], axis=0)
        outs = []
        for h in range(2):
            s = jnp.dot(q, keys[h, :, start:stop], preferred_element_type=F32)
            p = jnp.exp2(s - lifts[h][:, start:stop]).astype(BF16)
            outs.append(jnp.dot(p, vals[h, start:stop, :], preferred_element_type=F32))
        return outs

    def mix_near(slots):
        for h, out in enumerate(mix(slots, 0, near_keys)):
            for i, j in enumerate(slots):
                near_sum[h, j] = out[i * LANES : (i + 1) * LANES]

    def attend(slots, begun):
        outs = mix(slots, near_keys if begun else 0, nlat + LANES)
        for i, j in enumerate(slots):
            first, second = (out[i * LANES : (i + 1) * LANES] for out in outs)
            if begun:
                first, second = first + near_sum[0, j], second + near_sum[1, j]
            den = jnp.where(diagonal, jnp.where(low, second, first), 0.0)
            packed = jnp.concatenate(
                [
                    jnp.sum(den[:HD], axis=0, keepdims=True),
                    jnp.sum(den[HD:], axis=0, keepdims=True),
                ],
                axis=0,
            )
            hi = packed.astype(BF16).astype(F32)
            lo = packed - hi
            ostage[j, 0:LANES, :] = jnp.where(low, first, second).astype(BF16)
            ostage[j, LANES:, :] = jnp.concatenate([hi, lo, jnp.zeros((12, LANES), F32)], axis=0).astype(BF16)

    expand_slot(0)
    def relay(near, buf, whole, part, count, peer, first):
        if count < 8:
            return {}
        for k in (2, count - 2):
            near[k].wait_recv()
        out = {count // 2: []}
        for side, k, step in ((0, 2, 1), (1, count - 2, count - 1)):
            onward = (k + step) % count
            out[onward] = [remote(whole(buf.at[k]), whole(buf.at[onward]), first + onward, peer(step))]
        for side, k in ((0, 2), (1, count - 2)):
            out[count // 2].append(
                remote(part(buf.at[k], side), part(buf.at[count // 2], side), first + 8 + side, peer(k))
            )
        return out

    def key_whole(ref):
        return ref.at[core]

    def key_piece(ref, side):
        return ref.at[core, :, pl.ds(side * LANES, LANES)]

    def query_whole(ref):
        return ref

    def query_part(ref, side):
        return ref.at[pl.ds(side * (qrows // 2), qrows // 2), :]

    qrows = qbuf.shape[1]
    k_far = relay(k_near, msg, key_whole, key_piece, nz, z_peer, 96)
    q_far = relay(q_near, qbuf, query_whole, query_part, ny, y_peer, 112)
    arrivals = {k: [k_near[k]] for k in direct(nz)}
    arrivals.update(k_far)
    def take_keys(order):
        forwards = []
        for at, k in enumerate(order):
            landed(f for f in arrivals[k] if not f.landed)
            forwards.append(remote(msg.at[k, core], msg.at[k, core], 128 + k, sibling))
            if at > 0:
                forwards[at - 1].wait_recv()
                expand_slot(order[at - 1])
        if order:
            forwards[-1].wait_recv()
            expand_slot(order[-1])

    take_keys(direct(nz))
    near_slots = direct(ny) + [0]
    landed(q_near[k] for k in direct(ny) if not q_near[k].landed)
    for at in range(0, len(near_slots), 3):
        mix_near(near_slots[at : at + 3])
    take_keys(sorted(k_far, key=lambda k: min(k, nz - k)))

    latent = ctxl[...].astype(BF16)
    rope_k = ctxr[...].T[:ROPE]
    up = nt_dot(wupt[...], latent)
    shared = jnp.sum(rope_k * rope_k, axis=0, keepdims=True)
    at = pl.ds(nlat, LANES)
    for h in range(2):
        part = up[h * HD : (h + 1) * HD]
        inv = lax.rsqrt((jnp.sum(part * part, axis=0, keepdims=True) + shared) * (1.0 / QK) + EPS)
        keys[h, h * HD : (h + 1) * HD, at] = (part * inv * kg[:HD]).astype(BF16)
        keys[h, LANES + h * ROPE : LANES + (h + 1) * ROPE, at] = (rope_k * inv * kg[HD:QK]).astype(BF16)
    value = jnp.dot(latent, wup[1], preferred_element_type=F32)
    low = lane_ids((LANES, LANES)) < HD
    real = row_ids((LANES, LANES)) < nz * crow
    ones = jnp.where(real, 1.0, 0.0)
    vals[0, at, :] = jnp.where(low, value, ones).astype(BF16)
    vals[1, at, :] = jnp.where(low, ones, value).astype(BF16)

    o_copies = []
    o_half = []
    halves = ((0, HD), (HD, ostage.shape[1] - HD))
    groups = [(list(q_far), False)] if q_far else []
    tail_slots = near_slots[:-1]
    groups += [(tail_slots[at : at + 2], True) for at in range(0, len(tail_slots), 2)] or [([], True)]
    groups[-1][0].append(0)
    for slots, begun in groups:
        if not begun:
            landed(f for j in slots for f in q_far[j] if not f.landed)
        attend(slots, begun)
        for j in slots:
            if j == 4 and ny == 8:
                for side, step in ((0, 2), (1, ny - 2)):
                    rows_at = pl.ds(*halves[side])
                    o_half.append(
                        remote(ostage.at[j, rows_at, :], opass.at[rows_at, :], 138 + side, y_peer(step))
                    )
            elif j:
                o_copies.append(remote(ostage.at[j], obuf.at[j], 144 + j, y_peer(ny - j)))
    def pass_weights():
        for k in near_x:
            for flight in (w_first[k], w_second[k]):
                if not flight.landed:
                    flight.wait_recv()
            came = x_index(nx - k)
            w_side.append(remote(wout.at[came], wout.at[came], 175 + k, sibling))
        if w_far:
            landed(w_far)
            came = x_index(2)
            w_side.append(remote(wout.at[came], wout.at[came], 179, sibling))

    if o_half:
        for side, step in ((0, 2), (1, ny - 2)):
            o_half[side].wait_recv()
            rows_at = pl.ds(*halves[side])
            o_copies.append(remote(opass.at[rows_at, :], obuf.at[4, rows_at, :], 152 + side, y_peer(step)))
    pass_weights()
    landed(o_copies)
    num = ostage[0, 0:LANES, :].astype(F32)
    den = ostage[0, LANES:, :].astype(F32)
    for j in range(1, ny):
        num = num + obuf[j, 0:LANES, :].astype(F32)
        den = den + obuf[j, LANES:, :].astype(F32)
    den = den[0:2] + den[2:4]
    spread = jnp.concatenate(
        [
            jnp.broadcast_to(den[0:1], (HD, LANES)),
            jnp.broadcast_to(den[1:2], (HD, LANES)),
        ],
        axis=0,
    )
    spread = jnp.where(diagonal, spread, 0.0)
    swap = jnp.where((lane_ids((LANES, LANES)) < HD) != (row_ids((LANES, LANES)) < HD), 1.0, 0.0)
    spread = jnp.dot(spread, swap, precision=HIGHEST, preferred_element_type=F32)
    attended = (num / spread).astype(BF16)

    share_out[...] = attended.reshape(ntp, rows, LANES)
    heads[tp] = share_out[tp]
    a_copies = [
        remote(share_out.at[(tp + k) % ntp], heads.at[tp], 160 + k, t_peer(k)) for k in range(1, ntp)
    ]
    landed(w_side)
    landed(a_copies)
    mixed = jnp.concatenate([heads[t] for t in range(ntp)], axis=1)
    result = jnp.dot(mixed, wout[...].reshape(ntp * LANES, width), preferred_element_type=F32)
    landed(gt_copies)
    gate_row = jnp.concatenate([gtbuf[t] for t in range(ntp)], axis=1)
    out_ref[...] = (gtok[tp].astype(F32) + gate_row * result).astype(BF16)

    for flight in sent:
        flight.wait_send()


def solution(mesh, nz=8):
    nsp, ntp = mesh.shape["sp"], mesh.shape["tp"]
    ny = nsp // nz

    def local(
        latent_tokens,
        context_tokens,
        cond,
        ctx_cond,
        mod_shift,
        mod_scale,
        mod_gate,
        norm_gain,
        w_query,
        query_gain,
        w_down_kv,
        w_rope_key,
        kv_gain,
        w_up_kv,
        key_gain,
        ctx_lift,
        w_output,
    ):
        rows, width = latent_tokens.shape
        crow = context_tokens.shape[0]
        piece = mod_shift.shape[1]
        lat = nz * LANES
        vm = pltpu.VMEM
        anywhere = pl.BlockSpec(memory_space=pl.ANY)
        smem = pl.BlockSpec(memory_space=pltpu.SMEM)
        return pl.pallas_call(
            functools.partial(kernel, nz, ny, ntp),
            out_shape=jax.ShapeDtypeStruct((rows, width), BF16),
            in_specs=[anywhere] * 15 + [smem, anywhere],
            out_specs=pl.BlockSpec(memory_space=pltpu.VMEM),
            scratch_shapes=[
                vm((ntp, rows, width), BF16),
                vm((crow, width), BF16),
                vm((width // LANES, LANES), F32),
                vm((width // LANES, LANES), F32),
                vm((3, mod_shift.shape[0], piece), BF16),
                vm((1, width), F32),
                vm(w_query.shape[::-1], BF16),
                vm((1, QK), F32),
                vm(w_down_kv.shape, BF16),
                vm(w_rope_key.shape[::-1], BF16),
                vm((1, KVL), F32),
                vm(w_up_kv.shape, BF16),
                vm((1, QK), F32),
                vm((ntp, *w_output.shape), BF16),
                vm((nz, 2, 2 * piece), F32),
                vm((ny, 2, 2 * piece), F32),
                vm((ntp, 2, 2 * piece), F32),
                vm((nz, 1, piece), F32),
                vm((ny, 1, piece), F32),
                vm((ntp, 1, piece), F32),
                vm((LANES, width), F32),
                vm((crow, width), F32),
                vm((LANES + 16, width), BF16),
                vm((LANES, KVL), BF16),
                vm((nz, HALF, LANES), F32),
                vm((nz, HALF, LANES), F32),
                vm((nz, 2, MSG, KVL), BF16),
                vm((ny, LANES + HD, LANES), BF16),
                vm((2, 2 * LANES, lat + LANES), BF16),
                vm((2, lat + LANES, LANES), BF16),
                vm((2, ny, LANES, LANES), F32),
                vm((LANES, KVL), F32),
                vm((LANES, LANES), F32),
                vm((ny, LANES + 16, LANES), BF16),
                vm((ny, LANES + 16, LANES), BF16),
                vm((LANES + 16, LANES), BF16),
                vm((ntp, rows, LANES), BF16),
                vm((ntp, rows, LANES), BF16),
                pltpu.SemaphoreType.DMA((16,)),
                pltpu.SemaphoreType.DMA((184,)),
                pltpu.SemaphoreType.DMA((184,)),
            ],
            compiler_params=pltpu.CompilerParams(
                collective_id=0, has_side_effects=True, vmem_limit_bytes=60 * 1024 * 1024
            ),
        )(
            latent_tokens,
            context_tokens,
            cond.reshape(width // LANES, LANES),
            ctx_cond.reshape(width // LANES, LANES),
            mod_shift,
            mod_scale,
            mod_gate,
            norm_gain.reshape(1, width),
            w_query.T,
            query_gain.reshape(1, QK),
            w_down_kv,
            w_rope_key.T,
            kv_gain.reshape(1, KVL),
            w_up_kv,
            key_gain.reshape(1, QK),
            ctx_lift.reshape(1, 2),
            w_output,
        )

    in_specs = (
        P(("sp", "tp"), None),
        P("sp", None),
        P(),
        P(),
        P("sp", "tp"),
        P("sp", "tp"),
        P("sp", "tp"),
        P(),
        P(None, "tp"),
        P(),
        P(),
        P(),
        P(),
        P(None, None, "tp"),
        P(),
        P("tp"),
        P("tp", None),
    )
    return jax.shard_map(local, mesh=mesh, in_specs=in_specs, out_specs=P(("sp", "tp"), None), check_vma=False)
```

```python
import functools
import math

import jax
import jax.numpy as jnp
from jax import lax
from jax.experimental import pallas as pl
from jax.experimental.pallas import tpu as pltpu
from jax.sharding import PartitionSpec as P

HD = 64
ROPE = 32
QK = 96
KVL = 256
HALF = ROPE // 2
GRID_W = 64
EPS = 1e-06
THETA = 10000.0
LOG2E = math.log2(math.e)
MESH = pl.DeviceIdType.MESH
F32 = jnp.float32
BF16 = jnp.bfloat16
HIGHEST = lax.Precision.HIGHEST
LANES = 128
MSG = 80


def nt_dot(a, b):
    return lax.dot_general(a, b, (((1,), (1,)), ((), ())), preferred_element_type=F32)


def lane_ids(shape):
    return lax.broadcasted_iota(jnp.int32, shape, 1)


def row_ids(shape):
    return lax.broadcasted_iota(jnp.int32, shape, 0)


def silu(v):
    return v / (1.0 + jnp.exp(-v))


def column_tile(row):
    width = row.shape[1]
    full = jnp.concatenate([row, jnp.zeros((1, LANES - width), F32)], axis=1)
    return jnp.broadcast_to(full, (LANES, LANES)).T


class Flight:
    def __init__(self, sent, copy):
        self.copy, self.landed = copy, False
        sent.append(self)
        copy.start()

    def wait_recv(self):
        self.landed = True
        self.copy.wait_recv()

    def wait_send(self):
        self.copy.wait_send()


def angle_tables(group):
    shape = (HALF, LANES)
    freq_row = row_ids(shape)
    token = lane_ids(shape)
    inverse = jnp.zeros(shape, F32)
    for j in range(HALF // 2):
        inverse = jnp.where(freq_row % (HALF // 2) == j, THETA ** (-j / (HALF // 2)), inverse)
    row = (group * (LANES // GRID_W) + token // GRID_W).astype(F32)
    col = (token % GRID_W).astype(F32)
    angle = jnp.where(freq_row < HALF // 2, row, col) * inverse
    return jnp.cos(angle), jnp.sin(angle)


def rotated(tail, cosine, sine):
    front, back = tail[:HALF], tail[HALF:]
    return jnp.concatenate([front * cosine - back * sine, back * cosine + front * sine], axis=0)


def kernel(
    nz,
    ny,
    ntp,
    tok_h,
    ctx_h,
    cond_h,
    cctx_h,
    mshift_h,
    mscale_h,
    mgate_h,
    ngain_h,
    wq_h,
    qgain_h,
    wdown_h,
    wrope_h,
    kvgain_h,
    wup_h,
    kgain_h,
    lift_s,
    wout_h,
    out_ref,
    gtok,
    ctok,
    cond_v,
    cctx_v,
    mods,
    ngain,
    wq,
    qgain,
    wdown,
    wrope,
    kvgain,
    wup,
    kgain,
    wout,
    zbuf,
    ybuf,
    tbuf,
    gzbuf,
    gybuf,
    gtbuf,
    nv,
    nvc,
    hid,
    wupt,
    ctab,
    stab,
    msg,
    qbuf,
    keys,
    vals,
    ctxl,
    ctxr,
    ostage,
    obuf,
    dstage,
    dbuf,
    share_out,
    heads,
    load_sem,
    send_sem,
    recv_sem,
):
    sp = lax.axis_index("sp")
    tp = lax.axis_index("tp")
    zi, yi = sp // ny, sp % ny
    core = tp % 2
    rows = tok_h.shape[0]
    width = tok_h.shape[1]
    piece = mods.shape[2]
    crow = ctx_h.shape[0]
    nlat = nz * LANES

    def z_peer(k):
        return (((zi + k) % nz) * ny + yi, tp)

    def y_peer(k):
        return (zi * ny + (yi + k) % ny, tp)

    def t_peer(k):
        return (sp, (tp + k) % ntp)

    sibling = (sp, tp + 1 - 2 * core)

    def x_index(k):
        return (tp + 2 * k) % ntp

    def x_peer(k):
        return (sp, x_index(k))

    pairs = [
        (cond_h, cond_v),
        (cctx_h, cctx_v),
        (mshift_h, mods.at[0]),
        (mscale_h, mods.at[1]),
        (mgate_h, mods.at[2]),
        (tok_h, gtok.at[tp]),
        (ctx_h, ctok),
        (ngain_h, ngain),
        (wup_h, wup),
        (kgain_h, kgain),
        (qgain_h, qgain),
        (kvgain_h, kvgain),
        (wdown_h, wdown),
        (wrope_h, wrope),
        (wq_h, wq),
        (wout_h, wout.at[tp]),
    ]
    loads = [pltpu.make_async_copy(a, b, load_sem.at[i]) for i, (a, b) in enumerate(pairs)]
    for copy in loads:
        copy.start()

    barrier = pltpu.get_barrier_semaphore()
    peers = (
        [z_peer(k) for k in range(1, nz)]
        + [y_peer(k) for k in range(1, ny)]
        + [t_peer(k) for k in range(1, ntp)]
    )
    for peer in peers:
        pl.semaphore_signal(barrier, inc=1, device_id=peer, device_id_type=MESH)

    for i in range(5):
        loads[i].wait()
    mod_rows = mods.shape[1]
    fold = LANES // mod_rows
    quarter = sp % fold
    own_row = sp // fold
    lat_row = silu(cond_v[pl.ds(own_row, 1), :])
    ctx_row = silu(cctx_v[pl.ds(own_row, 1), :])
    mine = lane_ids((1, LANES)) // mod_rows == quarter
    signal = jnp.concatenate(
        [jnp.where(mine, lat_row, 0.0), jnp.where(mine, ctx_row, 0.0), jnp.zeros((6, LANES), F32)],
        axis=0,
    )
    block = jnp.concatenate([mods[0], mods[1], mods[2]], axis=1).astype(F32)
    block = jnp.concatenate([block] * fold, axis=0)
    share = jnp.dot(signal, block, precision=HIGHEST, preferred_element_type=F32)
    zbuf[0] = share[0:2, : 2 * piece]
    gzbuf[0] = share[0:1, 2 * piece :]

    pl.semaphore_wait(barrier, len(peers))

    sent = []

    def remote(src, dst, index, device):
        return Flight(
            sent,
            pltpu.make_async_remote_copy(
                src_ref=src,
                dst_ref=dst,
                send_sem=send_sem.at[index],
                recv_sem=recv_sem.at[index],
                device_id=device,
                device_id_type=MESH,
            ),
        )

    def far_first(count):
        return sorted(range(1, count), key=lambda k: -min(k, count - k))

    def exchange(buf, count, peer, first):
        return [remote(buf.at[0], buf.at[k], first + k, peer(k)) for k in far_first(count)]

    def spread_tp(buf, first):
        return [remote(buf.at[tp], buf.at[tp], first + k, t_peer(k)) for k in range(1, ntp)]

    def direct(count):
        if count < 8:
            return list(range(1, count))
        return [2, count - 2, 1, count - 1]

    def landed(flights):
        for flight in flights:
            flight.wait_recv()

    z_copies = exchange(zbuf, nz, z_peer, 0)
    gz_copies = exchange(gzbuf, nz, z_peer, 8)

    loads[5].wait()
    near_x = sorted({k for k in (1, ntp // 2 - 1) if 0 < k < ntp // 2})
    tok_near = {k: remote(gtok.at[tp], gtok.at[tp], 16 + k, x_peer(k)) for k in near_x}
    tok_side = [remote(gtok.at[tp], gtok.at[tp], 16, sibling)]
    tok_half = []

    for i in range(6, 12):
        loads[i].wait()
    gain_row = ngain[...]
    cv = ctok[...].astype(F32)
    nvc[...] = cv * lax.rsqrt(jnp.mean(cv * cv, axis=1, keepdims=True) + EPS) * gain_row
    wupt[...] = wup[0].astype(F32).T.astype(BF16)
    keys[...] = jnp.zeros(keys.shape, BF16)
    vals[:, nlat:, :] = jnp.zeros((2, LANES, LANES), BF16)
    ctxl[...] = jnp.zeros(ctxl.shape, F32)
    ctxr[...] = jnp.zeros(ctxr.shape, F32)
    msg[0, :, 64:80, :] = jnp.zeros((2, 16, KVL), BF16)
    hid[LANES:, :] = jnp.zeros((hid.shape[0] - LANES, width), BF16)
    kg = column_tile(kgain[...])
    qg = column_tile(qgain[...]) * (LOG2E * QK ** (-0.5))
    for k in range(nz):
        cosine, sine = angle_tables(((zi + nz - k) % nz) * ny + yi)
        ctab[k] = cosine
        stab[k] = sine

    for k in near_x:
        tok_near[k].wait_recv()
        came = x_index(ntp // 2 - k)
        if ntp // 2 == 4:
            lanes = pl.ds(0 if k == 1 else width // 2, width // 2)
            tok_half.append(
                remote(gtok.at[came, :, lanes], gtok.at[came, :, lanes], 20 + k, x_peer(k))
            )
        tok_side.append(remote(gtok.at[came], gtok.at[came], 24 + k, sibling))

    nx = ntp // 2
    half_w = width // 2

    def columns(side):
        return pl.ds(side * half_w, half_w)

    def w_block(index, side):
        return wout.at[index, :, columns(side)]

    loads[15].wait()
    w_side = [remote(wout.at[tp], wout.at[tp], 168, sibling)]
    w_first = {k: remote(w_block(tp, side), w_block(tp, side), 169 + side, x_peer(k)) for side, k in enumerate(near_x)}

    landed(z_copies)
    total = zbuf[0]
    for k in range(1, nz):
        total = total + zbuf[k]
    ybuf[0] = total
    y_copies = exchange(ybuf, ny, y_peer, 32)
    landed(gz_copies)
    total = gzbuf[0]
    for k in range(1, nz):
        total = total + gzbuf[k]
    gybuf[0] = total
    gy_copies = exchange(gybuf, ny, y_peer, 40)

    if tok_half:
        landed(tok_half)
        far = x_index(2)
        tok_side.append(remote(gtok.at[far], gtok.at[far], 28, sibling))
    landed(y_copies)
    total = ybuf[0]
    for k in range(1, ny):
        total = total + ybuf[k]
    tbuf[tp] = total

    t_copies = spread_tp(tbuf, 48)
    landed(gy_copies)
    total = gybuf[0]
    for k in range(1, ny):
        total = total + gybuf[k]
    gtbuf[tp] = total
    gt_copies = spread_tp(gtbuf, 56)

    landed(tok_side)

    def norm_rows(i, carry):
        v = gtok[i].astype(F32)
        scaled = v * lax.rsqrt(jnp.mean(v * v, axis=1, keepdims=True) + EPS) * gain_row
        nv[pl.ds(pl.multiple_of(i * rows, rows), rows), :] = scaled
        return carry

    lax.fori_loop(0, ntp, norm_rows, 0)

    for i in range(12, 15):
        loads[i].wait()
    landed(t_copies)
    w_second = {k: remote(w_block(tp, 1 - side), w_block(tp, 1 - side), 171 + side, x_peer(k)) for side, k in enumerate(near_x)}
    w_far = []
    if nx == 4:
        for side, k in enumerate(near_x):
            w_first[k].wait_recv()
            came = x_index(nx - k)
            w_far.append(remote(w_block(came, side), w_block(came, side), 173 + side, x_peer(k)))

    def vector(which, who):
        return jnp.concatenate(
            [tbuf[t][who : who + 1, which * piece : (which + 1) * piece] for t in range(ntp)],
            axis=1,
        )

    shift_row = vector(0, 0)
    scale_row = 1.0 + vector(1, 0)

    def modulate(i, carry):
        at = pl.ds(pl.multiple_of(i * 16, 16), 16)
        hid[at, :] = (nv[at, :] * scale_row + shift_row).astype(BF16)
        return carry

    lax.fori_loop(0, LANES // 16, modulate, 0)
    ctx_hidden = nvc[...] * (1.0 + vector(1, 1)) + vector(0, 1)
    hid[LANES : LANES + 16, :] = jnp.concatenate(
        [ctx_hidden, jnp.zeros((16 - crow, width), F32)], axis=0
    ).astype(BF16)

    raw = jnp.dot(hid[...], wdown[...], preferred_element_type=F32)
    lat = raw * lax.rsqrt(jnp.mean(raw * raw, axis=1, keepdims=True) + EPS) * kvgain[...]
    rope_t = nt_dot(wrope[...], hid[:LANES, :])
    rope_c = nt_dot(hid[LANES:, :], wrope[...])
    rope_c = jnp.concatenate([rope_c, jnp.zeros((16, LANES - ROPE), F32)], axis=1)
    ctx_lat = lat[LANES : LANES + crow]
    msg[0, 0, 0:64, :] = lat[0:64].astype(BF16)
    msg[0, 1, 0:64, :] = lat[64:128].astype(BF16)
    msg[0, 0, 64:80, 0:LANES] = rope_t[:16].astype(BF16)
    msg[0, 1, 64:80, 0:LANES] = rope_t[16:].astype(BF16)
    msg[0, 0, 64:80, LANES:] = jnp.concatenate([ctx_lat[:, :LANES], ctx_lat[:, LANES:]], axis=0).astype(BF16)
    msg[0, 1, 64:80, LANES:] = rope_c.astype(BF16)
    k_near = {
        k: remote(msg.at[0, core], msg.at[k, core], 64 + k, z_peer(k)) for k in direct(nz)
    }

    raw_t = nt_dot(wq[...], hid[:LANES, :])
    plains, tails = [], []
    for h in range(2):
        u = raw_t[h * QK : (h + 1) * QK]
        inv = lax.rsqrt(jnp.sum(u * u, axis=0, keepdims=True) * (1.0 / QK) + EPS)
        u = u * inv * qg[:QK]
        plains.append(u[:HD])
        tails.append(rotated(u[HD:], ctab[0], stab[0]))
    plain = jnp.concatenate(plains, axis=0).T
    tail = jnp.concatenate(tails, axis=0)
    tail = jnp.concatenate([tail, pltpu.roll(tail, LANES // 2, 1)], axis=0).T
    qbuf[0, 0:LANES, :] = plain.astype(BF16)
    qbuf[0, LANES:, :] = tail[: LANES // 2].astype(BF16)
    q_near = {k: remote(qbuf.at[0], qbuf.at[k], 80 + k, y_peer(k)) for k in direct(ny)}

    def expand_slot(k):
        latent = msg[k, :, 0:64, :].reshape(LANES, KVL)
        rope_k = jnp.concatenate([msg[k, 0, 64:80, 0:LANES], msg[k, 1, 64:80, 0:LANES]], axis=0).astype(F32)
        up = nt_dot(wupt[...], latent)
        shared = jnp.sum(rope_k * rope_k, axis=0, keepdims=True)
        at = pl.ds(k * LANES, LANES)
        for h in range(2):
            part = up[h * HD : (h + 1) * HD]
            inv = lax.rsqrt((jnp.sum(part * part, axis=0, keepdims=True) + shared) * (1.0 / QK) + EPS)
            keys[h, h * HD : (h + 1) * HD, at] = (part * inv * kg[:HD]).astype(BF16)
            turned = rotated(rope_k * inv * kg[HD:QK], ctab[k], stab[k])
            keys[h, LANES + h * ROPE : LANES + (h + 1) * ROPE, at] = turned.astype(BF16)
        value = jnp.dot(latent, wup[1], preferred_element_type=F32)
        low = lane_ids((LANES, LANES)) < HD
        vals[0, at, :] = jnp.where(low, value, 1.0).astype(BF16)
        vals[1, at, :] = jnp.where(low, 1.0, value).astype(BF16)
        ctx_two = msg[k, 0, 64:80, LANES:].astype(F32)
        ctxl[k * crow : (k + 1) * crow, :] = jnp.concatenate([ctx_two[:crow], ctx_two[8 : 8 + crow]], axis=1)
        ctxr[k * crow : (k + 1) * crow, :] = msg[k, 1, 64:80, LANES:].astype(F32)[:crow]

    expand_slot(0)
    def relay(near, buf, whole, part, count, peer, first):
        if count < 8:
            return {}
        for k in (2, count - 2):
            near[k].wait_recv()
        out = {count // 2: []}
        for side, k, step in ((0, 2, 1), (1, count - 2, count - 1)):
            onward = (k + step) % count
            out[onward] = [remote(whole(buf.at[k]), whole(buf.at[onward]), first + onward, peer(step))]
        for side, k in ((0, 2), (1, count - 2)):
            out[count // 2].append(
                remote(part(buf.at[k], side), part(buf.at[count // 2], side), first + 8 + side, peer(k))
            )
        return out

    def key_whole(ref):
        return ref.at[core]

    def key_part(ref, side):
        return ref.at[core, :, pl.ds(side * LANES, LANES)]

    def query_whole(ref):
        return ref

    def query_part(ref, side):
        return ref.at[pl.ds(side * (qrows // 2), qrows // 2), :]

    qrows = qbuf.shape[1]
    k_far = relay(k_near, msg, key_whole, key_part, nz, z_peer, 96)
    q_far = relay(q_near, qbuf, query_whole, query_part, ny, y_peer, 112)
    arrivals = {k: [k_near[k]] for k in direct(nz)}
    arrivals.update(k_far)
    forwards = []
    order = direct(nz) + sorted(k_far, key=lambda k: min(k, nz - k))
    for k in order:
        landed(f for f in arrivals[k] if not f.landed)
        forwards.append(remote(msg.at[k, core], msg.at[k, core], 128 + k, sibling))
        if len(forwards) > 1:
            forwards[-2].wait_recv()
            expand_slot(order[len(forwards) - 2])
    if forwards:
        forwards[-1].wait_recv()
        expand_slot(order[-1])

    latent = ctxl[...].astype(BF16)
    rope_k = ctxr[...].T[:ROPE]
    up = nt_dot(wupt[...], latent)
    shared = jnp.sum(rope_k * rope_k, axis=0, keepdims=True)
    at = pl.ds(nlat, LANES)
    for h in range(2):
        part = up[h * HD : (h + 1) * HD]
        inv = lax.rsqrt((jnp.sum(part * part, axis=0, keepdims=True) + shared) * (1.0 / QK) + EPS)
        keys[h, h * HD : (h + 1) * HD, at] = (part * inv * kg[:HD]).astype(BF16)
        keys[h, LANES + h * ROPE : LANES + (h + 1) * ROPE, at] = (rope_k * inv * kg[HD:QK]).astype(BF16)
    value = jnp.dot(latent, wup[1], preferred_element_type=F32)
    low = lane_ids((LANES, LANES)) < HD
    real = row_ids((LANES, LANES)) < nz * crow
    ones = jnp.where(real, 1.0, 0.0)
    vals[0, at, :] = jnp.where(low, value, ones).astype(BF16)
    vals[1, at, :] = jnp.where(low, ones, value).astype(BF16)

    diagonal = lane_ids((LANES, LANES)) % HD == row_ids((LANES, LANES)) % HD

    low = lane_ids((LANES, LANES)) < HD
    late = lane_ids((1, nlat + LANES)) < nlat
    lifts = [jnp.where(late, lift_s[0, h] * LOG2E, 0.0) for h in range(2)]

    def whole_query(j):
        tails = qbuf[j, LANES:, :]
        turned_tails = pltpu.roll(tails.astype(F32), LANES // 2, 1).astype(BF16)
        return jnp.concatenate([qbuf[j, 0:LANES, :], jnp.concatenate([tails, turned_tails], axis=0)], axis=1)

    def attend(slots):
        q = jnp.concatenate([whole_query(j) for j in slots], axis=0)
        outs = []
        for h in range(2):
            p = jnp.exp2(jnp.dot(q, keys[h], preferred_element_type=F32) - lifts[h]).astype(BF16)
            outs.append(jnp.dot(p, vals[h], preferred_element_type=F32))
        for i, j in enumerate(slots):
            first, second = (out[i * LANES : (i + 1) * LANES] for out in outs)
            den = jnp.where(diagonal, jnp.where(low, second, first), 0.0)
            packed = jnp.concatenate(
                [
                    jnp.sum(den[:HD], axis=0, keepdims=True),
                    jnp.sum(den[HD:], axis=0, keepdims=True),
                ],
                axis=0,
            )
            ostage[j, 0:LANES, :] = jnp.where(low, first, second).astype(BF16)
            dstage[j] = packed

    o_copies = []
    order = sorted(range(ny), key=lambda j: -min(j, ny - j))
    arrivals = {k: [q_near[k]] for k in direct(ny)}
    arrivals.update(q_far)
    arrivals[0] = []
    for at in range(0, ny, 2):
        slots = order[at : at + 2]
        for j in slots:
            landed(f for f in arrivals[j] if not f.landed)
        attend(slots)
        for j in slots:
            if j:
                o_copies.append(remote(dstage.at[j], dbuf.at[j], 184 + j, y_peer(ny - j)))
            if j:
                o_copies.append(remote(ostage.at[j], obuf.at[j], 144 + j, y_peer(ny - j)))
    def pass_weights():
        for k in near_x:
            for flight in (w_first[k], w_second[k]):
                if not flight.landed:
                    flight.wait_recv()
            came = x_index(nx - k)
            w_side.append(remote(wout.at[came], wout.at[came], 175 + k, sibling))
        if w_far:
            landed(w_far)
            came = x_index(2)
            w_side.append(remote(wout.at[came], wout.at[came], 179, sibling))

    pass_weights()
    landed(o_copies)
    num = ostage[0, 0:LANES, :].astype(F32)
    den = dstage[0]
    for j in range(1, ny):
        num = num + obuf[j, 0:LANES, :].astype(F32)
        den = den + dbuf[j]
    spread = jnp.concatenate(
        [
            jnp.broadcast_to(den[0:1], (HD, LANES)),
            jnp.broadcast_to(den[1:2], (HD, LANES)),
        ],
        axis=0,
    )
    spread = jnp.where(diagonal, spread, 0.0)
    swap = jnp.where((lane_ids((LANES, LANES)) < HD) != (row_ids((LANES, LANES)) < HD), 1.0, 0.0)
    spread = jnp.dot(spread, swap, precision=HIGHEST, preferred_element_type=F32)
    attended = (num / spread).astype(BF16)

    share_out[...] = attended.reshape(ntp, rows, LANES)
    heads[tp] = share_out[tp]
    a_copies = [
        remote(share_out.at[(tp + k) % ntp], heads.at[tp], 160 + k, t_peer(k)) for k in range(1, ntp)
    ]
    landed(w_side)
    landed(a_copies)
    mixed = jnp.concatenate([heads[t] for t in range(ntp)], axis=1)
    result = jnp.dot(mixed, wout[...].reshape(ntp * LANES, width), preferred_element_type=F32)
    landed(gt_copies)
    gate_row = jnp.concatenate([gtbuf[t] for t in range(ntp)], axis=1)
    out_ref[...] = (gtok[tp].astype(F32) + gate_row * result).astype(BF16)

    for flight in sent:
        flight.wait_send()


def solution(mesh, nz=8):
    nsp, ntp = mesh.shape["sp"], mesh.shape["tp"]
    ny = nsp // nz

    def local(
        latent_tokens,
        context_tokens,
        cond,
        ctx_cond,
        mod_shift,
        mod_scale,
        mod_gate,
        norm_gain,
        w_query,
        query_gain,
        w_down_kv,
        w_rope_key,
        kv_gain,
        w_up_kv,
        key_gain,
        ctx_lift,
        w_output,
    ):
        rows, width = latent_tokens.shape
        crow = context_tokens.shape[0]
        piece = mod_shift.shape[1]
        lat = nz * LANES
        vm = pltpu.VMEM
        anywhere = pl.BlockSpec(memory_space=pl.ANY)
        smem = pl.BlockSpec(memory_space=pltpu.SMEM)
        return pl.pallas_call(
            functools.partial(kernel, nz, ny, ntp),
            out_shape=jax.ShapeDtypeStruct((rows, width), BF16),
            in_specs=[anywhere] * 15 + [smem, anywhere],
            out_specs=pl.BlockSpec(memory_space=pltpu.VMEM),
            scratch_shapes=[
                vm((ntp, rows, width), BF16),
                vm((crow, width), BF16),
                vm((width // LANES, LANES), F32),
                vm((width // LANES, LANES), F32),
                vm((3, mod_shift.shape[0], piece), BF16),
                vm((1, width), F32),
                vm(w_query.shape[::-1], BF16),
                vm((1, QK), F32),
                vm(w_down_kv.shape, BF16),
                vm(w_rope_key.shape[::-1], BF16),
                vm((1, KVL), F32),
                vm(w_up_kv.shape, BF16),
                vm((1, QK), F32),
                vm((ntp, *w_output.shape), BF16),
                vm((nz, 2, 2 * piece), F32),
                vm((ny, 2, 2 * piece), F32),
                vm((ntp, 2, 2 * piece), F32),
                vm((nz, 1, piece), F32),
                vm((ny, 1, piece), F32),
                vm((ntp, 1, piece), F32),
                vm((LANES, width), F32),
                vm((crow, width), F32),
                vm((LANES + 16, width), BF16),
                vm((LANES, KVL), BF16),
                vm((nz, HALF, LANES), F32),
                vm((nz, HALF, LANES), F32),
                vm((nz, 2, MSG, KVL), BF16),
                vm((ny, LANES + HD, LANES), BF16),
                vm((2, 2 * LANES, lat + LANES), BF16),
                vm((2, lat + LANES, LANES), BF16),
                vm((LANES, KVL), F32),
                vm((LANES, LANES), F32),
                vm((ny, LANES, LANES), BF16),
                vm((ny, LANES, LANES), BF16),
                vm((ny, 2, LANES), F32),
                vm((ny, 2, LANES), F32),
                vm((ntp, rows, LANES), BF16),
                vm((ntp, rows, LANES), BF16),
                pltpu.SemaphoreType.DMA((16,)),
                pltpu.SemaphoreType.DMA((192,)),
                pltpu.SemaphoreType.DMA((192,)),
            ],
            compiler_params=pltpu.CompilerParams(
                collective_id=0, has_side_effects=True, vmem_limit_bytes=60 * 1024 * 1024
            ),
        )(
            latent_tokens,
            context_tokens,
            cond.reshape(width // LANES, LANES),
            ctx_cond.reshape(width // LANES, LANES),
            mod_shift,
            mod_scale,
            mod_gate,
            norm_gain.reshape(1, width),
            w_query.T,
            query_gain.reshape(1, QK),
            w_down_kv,
            w_rope_key.T,
            kv_gain.reshape(1, KVL),
            w_up_kv,
            key_gain.reshape(1, QK),
            ctx_lift.reshape(1, 2),
            w_output,
        )

    in_specs = (
        P(("sp", "tp"), None),
        P("sp", None),
        P(),
        P(),
        P("sp", "tp"),
        P("sp", "tp"),
        P("sp", "tp"),
        P(),
        P(None, "tp"),
        P(),
        P(),
        P(),
        P(),
        P(None, None, "tp"),
        P(),
        P("tp"),
        P("tp", None),
    )
    return jax.shard_map(local, mesh=mesh, in_specs=in_specs, out_specs=P(("sp", "tp"), None), check_vma=False)
```
